32 devices in a mesh: sp: 8 (over z, x), tp: 4 (over y, core).
Axes of the slice: x: 2, y: 2, z: 4, core: 2. Of those that a mesh axis runs over, the one named last changes fastest.
Arguments:
- cotangent: bfloat16 [2048, 2048], P('sp'), may hold values from -6 to 6
- route_ids: int32 [2048, 2], P('sp'), may hold values from 0 to 7, all different within a row; in each aligned block of 256 rows (0 to 255, 256 to 511, ...) at most 128 rows name the same one
- route_weights: float32 [2048, 2], P('sp'), may hold values from 0.2 to 1
- expert_inputs: bfloat16 [8, 1024, 2048], P('sp'), may hold values from -6 to 6
- gate_weight: bfloat16 [8, 2048, 1024], P('sp', None, 'tp'), may hold values from -0.125 to 0.125
- up_weight: bfloat16 [8, 2048, 1024], P('sp', None, 'tp'), may hold values from -0.125 to 0.125
- down_weight: bfloat16 [8, 1024, 2048], P('sp', 'tp'), may hold values from -0.1875 to 0.1875
- out_weight: bfloat16 [2048, 512], P(None, 'tp'), may hold values from -0.25 to 0.25
- gate_in: bfloat16 [2048, 512], P('sp', 'tp'), may hold values from -6 to 6
- conv_sum: bfloat16 [2048, 512], P('sp', 'tp'), may hold values from -6 to 6
- conv_c: bfloat16 [2048, 512], P('sp', 'tp'), may hold values from -6 to 6
- conv_v: bfloat16 [2048, 512], P('sp', 'tp'), may hold values from -6 to 6
- conv_taps: float32 [3, 512], P(None, 'tp'), may hold values from -3 to 3
Outputs:
- grad_input: bfloat16 [2048, 2048], P('sp', 'tp')
- grad_gate: bfloat16 [8, 2048, 1024], P('sp', None, 'tp')
- grad_up: bfloat16 [8, 2048, 1024], P('sp', None, 'tp')
- grad_down: bfloat16 [8, 1024, 2048], P('sp', 'tp')
- grad_out_weight: float32 [2048, 512], P('sp', 'tp')
- grad_gate_in: bfloat16 [2048, 512], P('sp', 'tp')
- grad_conv_c: bfloat16 [2048, 512], P('sp', 'tp')
- grad_conv_v: bfloat16 [2048, 512], P('sp', 'tp')
The draws below stay inside these ranges and needn't reach their ends.
Inputs may be any that keep to these rules, and one draw needn't show every extreme that they name: `route_ids`: the 2 experts of a token differ. Among the 256 tokens of one index of sp no expert is named more than 128 times, and in every draw some expert is named exactly 128 times by the tokens of some index of sp.
All inputs are finite; a program needn't handle non-finite values.
Results may differ from the reference program's by a relative error of at most 0.012.
Values may be sent and summed in bfloat16 or wider, within the bound.
No kernel may reach another device: no remote copies, remote signals or barrier semaphores. Data moves between devices by JAX's collectives and lax.ppermute only.
A program may use at most 128 MiB of HBM per device.

```python
import math
import jax
import jax.numpy as jnp
import numpy as np
from jax import lax

D = 2048
F = 1024
W = 512
TOP = 2
TAPS = 3
TOK_DEV = 256
EXPERTS = 8
CAP = 128
TOKENS = 2048
N_SP = 8
N_TP = 4


def spiked(result, rng, source, target, parts, factor):
    owner, partner = [(jnp.arange(result.shape[dim]) // (result.shape[dim] // parts)).reshape([-1 if axis == dim else 1 for axis in range(result.ndim)]) for dim in (source, target)]
    chosen = jax.random.permutation(rng, parts)[partner]
    strong = (owner == chosen) | (owner == (partner + parts // 2) % parts)
    return jnp.where(strong, factor * result, result)


def shard_levels(stream_key, extent, cuts, smallest, largest):
    def one(position, blocks):
        heights = jax.random.uniform(jax.random.fold_in(jax.random.fold_in(stream_key, 6), position), (blocks,), jnp.float32, smallest / len(cuts), largest / len(cuts))
        return jnp.repeat(jnp.exp(heights), extent[position] // blocks).reshape((-1,) + (1,) * (len(extent) - position - 1))

    gain = one(*cuts[0])
    for cut in cuts[1:]:
        gain = gain * one(*cut)
    return gain


def deal_out(own_key, own, number, rows, number_of, top, most, lean):
    order = jax.random.permutation(own_key, number_of)
    packed, ordinary = shares(number_of, rows * top, most, lean, True), shares(number_of, rows * top, most, lean, False)
    places = jnp.arange(number_of)

    def named(sizes, offset_by):
        used = int((sizes > 0).sum())
        fixed = max(1, used // 4)
        passed = fixed + (places - fixed + offset_by * (used - fixed)) % max(1, number_of - fixed)
        return jnp.zeros((number_of,), jnp.int32).at[order[jnp.where(places < fixed, places, passed)]].set(jnp.asarray(sizes, jnp.int32))

    sizes = jnp.where(number % 4 == 0, named(packed, number // 4), named(ordinary, number - number // 4 - 1))
    mixed = jax.random.permutation(jax.random.fold_in(own, 3), number_of)
    giver, receiver = mixed[0:number_of // 2 * 2:2], mixed[1:number_of // 2 * 2:2]
    room = jnp.minimum(sizes[giver] - 1, most - sizes[receiver]) // 2
    room = jnp.where((giver == order[0]) | (receiver == order[0]) | (sizes[receiver] == 0), 0, jnp.maximum(room, 0))
    passed = jax.random.randint(jax.random.fold_in(own, 4), (number_of // 2,), 0, 1 << 20) % (room + 1)
    sizes = sizes.at[giver].add(-passed).at[receiver].add(passed)
    labels = jnp.searchsorted(jnp.cumsum(sizes), jnp.arange(rows * top), side="right").astype(jnp.int32)
    table = labels.reshape(top, rows).T
    table = table[jax.random.permutation(jax.random.fold_in(own, 1), rows)]
    offset_by = jax.random.randint(jax.random.fold_in(own, 2), (rows, 1), 0, top)
    return jnp.take_along_axis(table, (jnp.arange(top)[None, :] + offset_by) % top, axis=1)


def shares(amount, total, bound, slope, full):
    loads = [(1 << 20) // math.isqrt(grade ** slope) + 1 for grade in range(1, amount + 1)]
    largest = bound if full else min(bound, max(-(-total // amount), total * loads[0] // sum(loads)))
    least = 1 if total - largest >= amount - 1 else 0
    counts, spare = [largest] + [least] * (amount - 1), total - largest - least * (amount - 1)
    while spare > 0:
        free = [i for i in range(1, amount) if counts[i] < largest] or [i for i in range(1, amount) if counts[i] < bound]
        mass, remaining = sum([loads[i] for i in free]), spare
        for i in free:
            more = min(bound - counts[i], max(1, remaining * loads[i] // mass), spare)
            counts[i] = counts[i] + more
            spare = spare - more
    return np.array(counts)


def scatter_about(stream_key, extent, scale, bound, split=(), kind=jnp.bfloat16):
    result = jax.random.normal(stream_key, extent, jnp.float32) * scale
    if len(split) > 0:
        result = shard_levels(stream_key, extent, split, -0.22, 0.18) * result
    return jnp.clip(result, min=-bound, max=bound).astype(kind)


def gaussian_with(own_key, extent, scale, limit, shards, heavy, held_as=jnp.bfloat16):
    array = scale * jax.random.normal(own_key, extent, jnp.float32)
    if shards:
        array = array * shard_levels(own_key, extent, shards, -0.22, 0.18)
    return jnp.clip(spiked(array, jax.random.fold_in(own_key, 3), *heavy), -limit, limit).astype(held_as)


def setup_inputs(seed: int = 0) -> dict:
    key_list = jax.random.split(jax.random.key(seed), 14)
    cotangent = gaussian_with(key_list[0], (TOKENS, D), 1.0, 6.0, ((0, 8),), (0, 1, 8, 2.0))
    route_ids_keys = jax.random.split(jax.random.fold_in(key_list[1], 1), TOKENS // TOK_DEV)
    route_ids_turns = jax.random.permutation(jax.random.fold_in(key_list[1], 3), TOKENS // TOK_DEV)
    route_ids = jax.vmap(lambda own, number: deal_out(jax.random.fold_in(key_list[1], 2), own, number, TOK_DEV, EXPERTS, TOP, CAP, 1))(route_ids_keys, route_ids_turns).reshape((TOKENS, TOP))
    route_weights = jnp.clip(0.2 + 0.8 * jax.random.uniform(key_list[2], (TOKENS, TOP), jnp.float32) ** shard_levels(key_list[2], (TOKENS, TOP), ((0, 8),), -0.2, 0.2), 0.2, 1.0)
    expert_inputs = scatter_about(key_list[3], (EXPERTS, N_SP * CAP, D), 1.0, 6.0, ((0, 8),))
    gate_weight = scatter_about(key_list[4], (EXPERTS, D, F), D ** -0.5, 0.125, ((0, 8), (2, 4)))
    up_weight = scatter_about(key_list[5], (EXPERTS, D, F), D ** -0.5, 0.125, ((0, 8), (2, 4)))
    down_weight = scatter_about(key_list[6], (EXPERTS, F, D), F ** -0.5, 0.1875, ((0, 8), (1, 4)))
    out_weight = scatter_about(key_list[7], (D, W), W ** -0.5, 0.25, ((1, 4),))
    gate_in = scatter_about(key_list[8], (TOKENS, W), 1.0, 6.0, ((0, 8), (1, 4)))
    conv_sum = scatter_about(key_list[9], (TOKENS, W), 1.0, 6.0, ((0, 8), (1, 4)))
    conv_c = scatter_about(key_list[10], (TOKENS, W), 1.0, 6.0, ((0, 8), (1, 4)))
    conv_v = scatter_about(key_list[11], (TOKENS, W), 1.0, 6.0, ((0, 8), (1, 4)))
    conv_taps = scatter_about(key_list[12], (TAPS, W), 0.6, 3.0, ((1, 4),), jnp.float32)
    return dict(cotangent=cotangent, route_ids=route_ids, route_weights=route_weights, expert_inputs=expert_inputs, gate_weight=gate_weight, up_weight=up_weight, down_weight=down_weight, out_weight=out_weight, gate_in=gate_in, conv_sum=conv_sum, conv_c=conv_c, conv_v=conv_v, conv_taps=conv_taps)


def reference(cotangent, route_ids, route_weights, expert_inputs, gate_weight, up_weight, down_weight, out_weight, gate_in, conv_sum, conv_c, conv_v, conv_taps):
    experts = gate_weight.shape[0]
    pair_ids = route_ids.reshape(N_SP, TOK_DEV * TOP)
    onehot = (pair_ids[:, :, None] == jnp.arange(experts, dtype=jnp.int32)[None, None, :]).astype(jnp.int32)
    before = jnp.cumsum(onehot, axis=1) - onehot
    ranked = jnp.sum(before * onehot, axis=2)
    source = jnp.arange(N_SP, dtype=jnp.int32)[:, None]
    slot_row = (source * CAP + ranked).reshape(-1).astype(jnp.int32)
    target = pair_ids.reshape(-1).astype(jnp.int32)
    weighted = (route_weights[:, :, None] * cotangent.astype(jnp.float32)[:, None, :]).astype(jnp.bfloat16).reshape(-1, D)
    routed = jnp.zeros((experts, N_SP * CAP, D), jnp.bfloat16).at[target, slot_row].set(weighted)
    quarter = F // N_TP

    def expert_step(expert_items):
        stored, grad_rows, w_gate, w_up, w_down = expert_items
        pre_gate = jnp.dot(stored, w_gate, preferred_element_type=jnp.float32)
        pre_up = jnp.dot(stored, w_up, preferred_element_type=jnp.float32)
        gate_sig = jax.nn.sigmoid(pre_gate)
        swish_gate = pre_gate * gate_sig
        hidden = (swish_gate * pre_up).astype(jnp.bfloat16)
        grad_hidden = jnp.dot(grad_rows, w_down.T, preferred_element_type=jnp.float32)
        grad_pregate = (grad_hidden * pre_up * gate_sig * (1.0 + pre_gate * (1.0 - gate_sig))).astype(jnp.bfloat16)
        grad_preup = (grad_hidden * swish_gate).astype(jnp.bfloat16)
        grad_down = jnp.dot(hidden.T, grad_rows, preferred_element_type=jnp.float32).astype(jnp.bfloat16)
        grad_gate = jnp.dot(stored.T, grad_pregate, preferred_element_type=jnp.float32).astype(jnp.bfloat16)
        grad_up = jnp.dot(stored.T, grad_preup, preferred_element_type=jnp.float32).astype(jnp.bfloat16)
        total = jnp.zeros((stored.shape[0], D), jnp.float32)
        for part_index in range(N_TP):
            low = part_index * quarter
            high = low + quarter
            part = jnp.dot(grad_pregate[:, low:high], w_gate[:, low:high].T, preferred_element_type=jnp.float32)
            part = part + jnp.dot(grad_preup[:, low:high], w_up[:, low:high].T, preferred_element_type=jnp.float32)
            total = total + lax.optimization_barrier(part.astype(jnp.bfloat16)).astype(jnp.float32)
        return grad_gate, grad_up, grad_down, total.astype(jnp.bfloat16)

    grad_gate, grad_up, grad_down, grad_x = lax.map(expert_step, (expert_inputs, routed, gate_weight, up_weight, down_weight))
    returned = grad_x[target, slot_row].astype(jnp.float32).reshape(TOKENS, TOP, D)
    grad_input = (cotangent.astype(jnp.float32) + jnp.sum(returned, axis=1)).astype(jnp.bfloat16)
    mixed_rows = (gate_in.astype(jnp.float32) * conv_sum.astype(jnp.float32)).astype(jnp.bfloat16)
    grad_mixed = jnp.dot(grad_input, out_weight, preferred_element_type=jnp.float32)
    grad_out_weight = jnp.dot(grad_input.T, mixed_rows, preferred_element_type=jnp.float32)
    grad_gate_in = (grad_mixed * conv_sum.astype(jnp.float32)).astype(jnp.bfloat16)
    grad_sum = grad_mixed * gate_in.astype(jnp.float32)
    extended = jnp.concatenate([grad_sum, jnp.zeros((2, grad_sum.shape[1]), jnp.float32)], axis=0)
    grad_prod = conv_taps[0] * extended[2:] + conv_taps[1] * extended[1:-1] + conv_taps[2] * extended[:-2]
    grad_conv_c = (grad_prod * conv_v.astype(jnp.float32)).astype(jnp.bfloat16)
    grad_conv_v = (grad_prod * conv_c.astype(jnp.float32)).astype(jnp.bfloat16)
    return (grad_input, grad_gate, grad_up, grad_down, grad_out_weight, grad_gate_in, grad_conv_c, grad_conv_v)
```

```python
import functools

import jax
import jax.numpy as jnp
from jax import lax
from jax.experimental import pallas as pl
from jax.experimental.pallas import tpu as pltpu
from jax.sharding import PartitionSpec as P


F32 = jnp.float32
BF16 = jnp.bfloat16
VMEM_LIMIT = 56 * 1024 * 1024


def dot(a, b, contract):
    return lax.dot_general(a, b, (contract, ((), ())), preferred_element_type=F32)


def whole(shape):
    return pl.BlockSpec(shape, lambda *_: (0,) * len(shape))


def params():
    return pltpu.CompilerParams(vmem_limit_bytes=VMEM_LIMIT)


def swap(value, axis, distance):
    route = [(i, i ^ distance) for i in range(lax.axis_size(axis))]
    return lax.ppermute(value, axis, route)


def dispatch_kernel(lanes, capacity, own_first, info, ids, weights, cot, select, *blocks):
    slots, tokens = select.shape
    model_width = cot.shape[1]
    cols = model_width // lanes
    experts = slots // capacity
    lane = info[1]
    labels = ids[...] ^ info[0]
    expert = lax.broadcasted_iota(jnp.int32, (experts, tokens), 0)
    hit = jnp.zeros((experts, tokens), F32)
    factor = jnp.zeros((experts, tokens), F32)
    for k in range(labels.shape[0]):
        same = expert == labels[k : k + 1]
        hit = hit + same.astype(F32)
        factor = factor + jnp.where(same, weights[k : k + 1], 0.0)
    earlier = (
        lax.broadcasted_iota(jnp.int32, (tokens, tokens), 0)
        < lax.broadcasted_iota(jnp.int32, (tokens, tokens), 1)
    ).astype(F32)
    before = dot(hit.astype(BF16), earlier.astype(BF16), ((1,), (0,))).astype(jnp.int32)
    rank = jnp.where(hit > 0, before, -1)
    row = lax.broadcasted_iota(jnp.int32, (experts, capacity, tokens), 1)
    chosen = (rank[:, None, :] == row).astype(F32)
    scale = jnp.sum(chosen * factor[:, None, :], axis=2, keepdims=True).reshape(slots, 1)
    matrix = chosen.reshape(slots, tokens).astype(BF16)
    select[...] = matrix

    def columns(index):
        return cot[:, pl.ds(pl.multiple_of(index * cols, cols), cols)]

    rows = (dot(matrix, columns(lane), ((1,), (0,))) * scale).astype(BF16)
    if own_first:
        for k in range(experts):
            blocks[k][...] = rows[k * capacity : (k + 1) * capacity]
        for j in range(1, lanes):
            part = dot(matrix[:capacity], columns(lane ^ j), ((1,), (0,)))
            blocks[experts + j - 1][...] = (part * scale[:capacity]).astype(BF16)
    else:
        blocks[0][...] = rows


def pre_kernel(info, x, w_gate, w_up, hidden, slope, swish):
    gate = dot(x[...], w_gate[...], ((1,), (0,)))
    up = dot(x[...], w_up[...], ((1,), (0,)))
    sig = jax.nn.sigmoid(gate)
    silu = gate * sig
    hidden[...] = (silu * up).astype(BF16)
    slope[...] = up * sig * (1.0 + gate * (1.0 - sig))
    swish[...] = silu


def mid_kernel(lanes, info, slope, swish, w_gate, w_up, w_down, *refs):
    pieces, (d_gate, d_up), outs = refs[:lanes], refs[lanes : lanes + 2], refs[lanes + 2 :]
    cols = w_gate.shape[0] // lanes
    lane = info[1]

    def spot(j):
        return pl.ds(pl.multiple_of((lane ^ j) * cols, cols), cols)

    total = dot(pieces[0][...], w_down[:, spot(0)], ((1,), (1,)))
    for j in range(1, lanes):
        total = total + dot(pieces[j][...], w_down[:, spot(j)], ((1,), (1,)))
    gate = (total * slope[...]).astype(BF16)
    up = (total * swish[...]).astype(BF16)
    d_gate[...] = gate
    d_up[...] = up
    for j in range(lanes):
        part = dot(gate, w_gate[spot(j), :], ((1,), (1,)))
        part = part + dot(up, w_up[spot(j), :], ((1,), (1,)))
        outs[j][...] = part.astype(BF16)


def down_kernel(lanes, count, info, hidden, *refs):
    pieces, out = refs[:-1], refs[-1]
    cols = out.shape[1] // lanes
    lane = info[1]
    for j in range(lanes):
        total = None
        start = 0
        for g in range(count):
            piece = pieces[g * lanes + j]
            size = piece.shape[0]
            term = dot(hidden[start : start + size], piece[...], ((0,), (0,)))
            total = term if total is None else total + term
            start += size
        spot = pl.ds(pl.multiple_of((lane ^ j) * cols, cols), cols)
        out[:, spot] = total.astype(BF16)


def gate_up_kernel(capacity, count, info, x, *refs):
    grads, (out_gate, out_up) = refs[: 2 * count], refs[2 * count :]
    order = info[2]
    gates, ups = None, None
    k = 0
    for g in range(count):
        gate, up = grads[2 * g], grads[2 * g + 1]
        for i in range(gate.shape[0] // capacity):
            spot = pl.ds(pl.multiple_of((order ^ k) * capacity, capacity), capacity)
            part = slice(i * capacity, (i + 1) * capacity)
            rows = x[spot, :]
            one = dot(rows, gate[part], ((0,), (0,)))
            two = dot(rows, up[part], ((0,), (0,)))
            gates = one if gates is None else gates + one
            ups = two if ups is None else ups + two
            k += 1
    out_gate[...] = gates.astype(BF16)
    out_up[...] = ups.astype(BF16)


def combine_kernel(info, select, cot, *refs):
    blocks, out = refs[:-1], refs[-1]
    total = cot[...].astype(F32)
    start = 0
    for block in blocks:
        size = block.shape[0]
        total = total + dot(select[start : start + size], block[...], ((0,), (0,)))
        start += size
    out[...] = total.astype(BF16)


def mixer_kernel(lanes, split, info, gate_in, conv_sum, w_out, *refs):
    pieces = refs[:lanes]
    d_gate_in, d_sum = refs[lanes : lanes + 2]
    own, outs, scratch = refs[lanes + 2], refs[lanes + 3 : -1], refs[-1]
    cols = pieces[0].shape[1]
    lane, order = info[1], info[2]
    gate = gate_in[...].astype(F32)
    conv = conv_sum[...].astype(F32)
    mixed = (gate * conv).astype(BF16)
    total = None
    for j in range(lanes):
        spot = pl.ds(pl.multiple_of((lane ^ j) * cols, cols), cols)
        piece = pieces[j][...]
        term = dot(piece, w_out[spot, :], ((1,), (0,)))
        total = term if total is None else total + term
        scratch[spot, :] = dot(piece, mixed, ((0,), (0,)))
    d_gate_in[...] = (total * conv).astype(BF16)
    d_sum[...] = total * gate
    size = own.shape[0]
    if split:
        for k in range(scratch.shape[0] // size):
            part = scratch[pl.ds(pl.multiple_of((order ^ k) * size, size), size), :]
            if k == 0:
                own[...] = part
            else:
                outs[k - 1][...] = part.astype(BF16)
    else:
        own[...] = scratch[pl.ds(pl.multiple_of(info[3] * size, size), size), :]
        outs[0][...] = scratch[...].astype(BF16)


def call(kernel, info, grid, ins, in_specs, out_shapes, out_specs, scratch=(), name=None):
    return pl.pallas_call(
        kernel,
        grid_spec=pltpu.PrefetchScalarGridSpec(
            num_scalar_prefetch=1,
            grid=grid,
            in_specs=in_specs,
            out_specs=out_specs,
            scratch_shapes=list(scratch),
        ),
        out_shape=out_shapes,
        compiler_params=params(),
        name=name,
    )(info, *ins)


def struct(shape, dtype):
    return jax.ShapeDtypeStruct(shape, dtype)


def gather_lanes(own, lanes):
    pieces = [own]
    distance = lanes // 2
    have = {0: own}
    while distance >= 1:
        for j in list(have):
            have[j ^ distance] = swap(have[j], "tp", distance)
        distance //= 2
    return [have[j] for j in range(lanes)]


def sum_lanes(parts, lanes):
    have = {j: parts[j].astype(F32) for j in range(lanes)}
    distance = 1
    while distance < lanes:
        sent = {j: swap(have[j].astype(BF16), "tp", distance) for j in have if j & distance}
        have = {
            j: have[j] + sent[j ^ distance].astype(F32) for j in have if not j & distance
        }
        distance *= 2
    return have[0].astype(BF16)


def body(
    cotangent,
    route_ids,
    route_weights,
    expert_inputs,
    gate_weight,
    up_weight,
    down_weight,
    out_weight,
    gate_in,
    conv_sum,
    conv_c,
    conv_v,
    conv_taps,
):
    groups = lax.axis_size("sp")
    lanes = lax.axis_size("tp")
    capacity = expert_inputs.shape[1] // groups
    tokens, model_width = cotangent.shape
    cols = model_width // lanes
    units = gate_weight.shape[2]
    slots = groups * capacity
    channels = gate_in.shape[1]
    part_rows = model_width // groups
    if gate_weight.shape[0] != 1 or lanes & (lanes - 1):
        raise ValueError("unsupported mesh")
    direct = groups == 8
    me, lane = lax.axis_index("sp"), lax.axis_index("tp")
    order = me if direct else jnp.zeros_like(me)
    info = jnp.stack([order, lane, order, me]).astype(jnp.int32)
    x = expert_inputs[0]
    w_gate, w_up, w_down = gate_weight[0], up_weight[0], down_weight[0]
    members = [[0], [1, 2, 3], [4, 5], [6, 7]] if direct else [list(range(groups))]

    block = struct((capacity, cols), BF16)
    if direct:
        shapes = [block] * (groups + lanes - 1)
    else:
        shapes = [struct((slots, cols), BF16)]
    select, *blocks = call(
        functools.partial(dispatch_kernel, lanes, capacity, direct),
        info,
        (1,),
        (route_ids.T, route_weights.T, cotangent),
        [whole(route_ids.T.shape), whole(route_ids.T.shape), whole(cotangent.shape)],
        [struct((slots, tokens), BF16)] + shapes,
        [whole((slots, tokens))] + [whole(s.shape) for s in shapes],
        name="dispatch",
    )
    hidden, slope, swish = call(
        pre_kernel,
        info,
        (groups,),
        (x, w_gate, w_up),
        [
            pl.BlockSpec((capacity, model_width), lambda k, info: (info[2] ^ k, 0)),
            whole(w_gate.shape),
            whole(w_up.shape),
        ],
        [struct((slots, units), BF16), struct((slots, units), F32), struct((slots, units), F32)],
        [pl.BlockSpec((capacity, units), lambda k, info: (k, 0))] * 3,
        name="pre",
    )

    def arrive(ks):
        if not direct:
            value = blocks[0].reshape(groups, capacity, cols)
            value = lax.all_to_all(value, "sp", split_axis=0, concat_axis=0, tiled=True)
            return gather_lanes(value.reshape(slots, cols), lanes)
        if ks == [0]:
            return [blocks[0]] + blocks[groups:]
        got = [swap(blocks[k], "sp", k) for k in ks]
        return gather_lanes(jnp.concatenate(got, axis=0), lanes)

    arrived = {}
    for g in reversed(range(len(members))):
        arrived[g] = arrive(members[g])

    grads, returned = {}, {}
    for g, ks in enumerate(members):
        first = ks[0]
        span = struct((len(ks) * capacity, units), BF16)
        wide = struct((len(ks) * capacity, cols), BF16)
        step = pl.BlockSpec((capacity, cols), lambda i, info: (i, 0))
        near = pl.BlockSpec((capacity, units), lambda i, info: (i, 0))
        rest = pl.BlockSpec((capacity, units), functools.partial(lambda f, i, info: (f + i, 0), first))
        gate, up, *parts = call(
            functools.partial(mid_kernel, lanes),
            info,
            (len(ks),),
            (slope, swish, w_gate, w_up, w_down, *arrived[g]),
            [rest, rest, whole(w_gate.shape), whole(w_up.shape), whole(w_down.shape)]
            + [step] * lanes,
            [span, span] + [wide] * lanes,
            [near, near] + [step] * lanes,
            name="mid%d" % g,
        )
        grads[g] = (gate, up)
        total = sum_lanes(parts, lanes)
        if not direct:
            total = total.reshape(groups, capacity, cols)
            total = lax.all_to_all(total, "sp", split_axis=0, concat_axis=0, tiled=True)
            returned[0] = total.reshape(slots, cols)
        else:
            for i, k in enumerate(ks):
                one = total[i * capacity : (i + 1) * capacity]
                returned[k] = swap(one, "sp", k) if k else one

    count = len(members)
    flat = [piece for g in range(count) for piece in arrived[g]]
    (grad_down,) = call(
        functools.partial(down_kernel, lanes, count),
        info,
        (1,),
        (hidden, *flat),
        [whole(hidden.shape)] + [whole(p.shape) for p in flat],
        [struct((units, model_width), BF16)],
        [whole((units, model_width))],
        name="grad_down",
    )
    flat = [grad for g in range(count) for grad in grads[g]]
    grad_gate, grad_up = call(
        functools.partial(gate_up_kernel, capacity, count),
        info,
        (1,),
        (x, *flat),
        [whole(x.shape)] + [whole(p.shape) for p in flat],
        [struct((model_width, units), BF16)] * 2,
        [whole((model_width, units))] * 2,
        name="grad_gate_up",
    )

    blocks = [returned[k] for k in sorted(returned)]
    (grad_input,) = call(
        combine_kernel,
        info,
        (1,),
        (select, cotangent, *blocks),
        [whole(select.shape), pl.BlockSpec((tokens, cols), lambda i, info: (0, info[1]))]
        + [whole(b.shape) for b in blocks],
        [struct((tokens, cols), BF16)],
        [whole((tokens, cols))],
        name="combine",
    )
    pieces = gather_lanes(grad_input, lanes)
    part = struct((part_rows, channels), BF16)
    outs = [part] * (groups - 1) if direct else [struct((model_width, channels), BF16)]
    shapes = [
        struct((tokens, channels), BF16),
        struct((tokens, channels), F32),
        struct((part_rows, channels), F32),
    ] + outs
    grad_gate_in, grad_sum, own, *terms = call(
        functools.partial(mixer_kernel, lanes, direct),
        info,
        (1,),
        (gate_in, conv_sum, out_weight, *pieces),
        [whole(gate_in.shape), whole(conv_sum.shape), whole(out_weight.shape)]
        + [whole(p.shape) for p in pieces],
        shapes,
        [whole(s.shape) for s in shapes],
        scratch=[pltpu.VMEM((model_width, channels), F32)],
        name="mixer",
    )
    back = [(i, i - 1) for i in range(1, groups)]
    next_rows = lax.ppermute(grad_sum[:2], "sp", back)
    if direct:
        grad_out_weight = own
        for k in range(1, groups):
            grad_out_weight = grad_out_weight + swap(terms[k - 1], "sp", k).astype(F32)
    else:
        value = terms[0].reshape(groups, part_rows, channels)
        value = lax.all_to_all(value, "sp", split_axis=0, concat_axis=0, tiled=True)
        others = (jnp.arange(groups) != me)[:, None, None]
        grad_out_weight = own + jnp.sum(jnp.where(others, value.astype(F32), 0.0), axis=0)
    extended = jnp.concatenate([grad_sum, next_rows], axis=0)
    grad_prod = (
        conv_taps[0] * extended[2:] + conv_taps[1] * extended[1:-1] + conv_taps[2] * extended[:-2]
    )
    grad_conv_c = (grad_prod * conv_v.astype(F32)).astype(BF16)
    grad_conv_v = (grad_prod * conv_c.astype(F32)).astype(BF16)
    return (
        grad_input,
        grad_gate[None],
        grad_up[None],
        grad_down[None],
        grad_out_weight,
        grad_gate_in,
        grad_conv_c,
        grad_conv_v,
    )


def solution(mesh):
    placed = (
        P("sp", None),
        P("sp", None),
        P("sp", None),
        P("sp", None, None),
        P("sp", None, "tp"),
        P("sp", None, "tp"),
        P("sp", "tp", None),
        P(None, "tp"),
        P("sp", "tp"),
        P("sp", "tp"),
        P("sp", "tp"),
        P("sp", "tp"),
        P(None, "tp"),
    )
    return jax.shard_map(
        body,
        mesh=mesh,
        in_specs=placed,
        out_specs=(
            P("sp", "tp"),
            P("sp", None, "tp"),
            P("sp", None, "tp"),
            P("sp", "tp", None),
            P("sp", "tp"),
            P("sp", "tp"),
            P("sp", "tp"),
            P("sp", "tp"),
        ),
        check_vma=False,
    )
```

```python
import functools

import jax
import jax.numpy as jnp
from jax import lax
from jax.experimental import pallas as pl
from jax.experimental.pallas import tpu as pltpu
from jax.sharding import PartitionSpec as P


F32 = jnp.float32
BF16 = jnp.bfloat16


def dot(a, b, contract):
    return lax.dot_general(a, b, (contract, ((), ())), preferred_element_type=F32)


def swap(value, axis, distance):
    route = [(i, i ^ distance) for i in range(lax.axis_size(axis))]
    return lax.ppermute(value, axis, route)


def position(direct):
    me = lax.axis_index("sp")
    return (me if direct else 0), me, lax.axis_index("tp")


def routing(ids, weights, experts, capacity, order):
    tokens = ids.shape[1]
    slots = experts * capacity
    labels = ids[...] ^ order
    expert = lax.broadcasted_iota(jnp.int32, (experts, tokens), 0)
    hit = jnp.zeros((experts, tokens), F32)
    factor = jnp.zeros((experts, tokens), F32)
    for k in range(labels.shape[0]):
        same = expert == labels[k : k + 1]
        hit = hit + same.astype(F32)
        factor = factor + jnp.where(same, weights[k : k + 1], 0.0)
    earlier = (
        lax.broadcasted_iota(jnp.int32, (tokens, tokens), 0)
        < lax.broadcasted_iota(jnp.int32, (tokens, tokens), 1)
    ).astype(F32)
    before = dot(hit.astype(BF16), earlier.astype(BF16), ((1,), (0,))).astype(jnp.int32)
    rank = jnp.where(hit > 0, before, -1)
    row = lax.broadcasted_iota(jnp.int32, (experts, capacity, tokens), 1)
    chosen = (rank[:, None, :] == row).astype(F32)
    scale = jnp.sum(chosen * factor[:, None, :], axis=2, keepdims=True).reshape(slots, 1)
    return chosen.reshape(slots, tokens), scale


def lane_columns_of(ref, lane, cols):
    return ref.at[:, pl.ds(pl.multiple_of(lane * cols, cols), cols)]


def in_hbm(*arrays):
    return [pltpu.with_memory_space_constraint(a, pltpu.HBM) for a in arrays]


def lane_columns(ref, lane, cols):
    return ref[:, pl.ds(pl.multiple_of(lane * cols, cols), cols)]


def dispatch_kernel(experts, direct, ids_in, weights_in, cot_in, *refs):
    blocks, (ids, weights, cot, sems) = refs[:-4], refs[-4:]
    order, _, lane = position(direct)
    capacity = blocks[0].shape[0] if direct else blocks[0].shape[0] // experts
    cols = cot.shape[1]
    copies = [
        pltpu.make_async_copy(ids_in, ids, sems.at[0]),
        pltpu.make_async_copy(weights_in, weights, sems.at[1]),
        pltpu.make_async_copy(lane_columns_of(cot_in, lane, cols), cot, sems.at[2]),
    ]
    for copy in copies:
        copy.start()
    copies[0].wait()
    copies[1].wait()
    chosen, scale = routing(ids, weights, experts, capacity, order)
    copies[2].wait()
    rows = dot(chosen.astype(BF16), cot[...], ((1,), (0,))) * scale
    if direct:
        for k in range(1, experts):
            blocks[k - 1][...] = rows[k * capacity : (k + 1) * capacity].astype(BF16)
    else:
        blocks[0][...] = rows.astype(BF16)


def local_kernel(lanes, experts, capacity, direct, ids_in, weights_in, cot_in, *refs):
    select, own_cot, *pieces = refs[:-4]
    ids, weights, cot, sems = refs[-4:]
    order, _, lane = position(direct)
    cols = cot.shape[1] // lanes
    copies = [
        pltpu.make_async_copy(ids_in, ids, sems.at[0]),
        pltpu.make_async_copy(weights_in, weights, sems.at[1]),
        pltpu.make_async_copy(cot_in, cot, sems.at[2]),
    ]
    for copy in copies:
        copy.start()
    for copy in copies:
        copy.wait()
    chosen, scale = routing(ids, weights, experts, capacity, order)
    select[...] = chosen.T.astype(BF16)
    own_cot[...] = lane_columns(cot, lane, cols)
    if direct:
        first = chosen[:capacity].astype(BF16)
        for j in range(lanes):
            rows = dot(first, lane_columns(cot, lane ^ j, cols), ((1,), (0,)))
            pieces[j][...] = (rows * scale[:capacity]).astype(BF16)


def pre_kernel(capacity, info, x, w_gate, w_up, hidden, slope, swish):
    gate = dot(x[...], w_gate[...], ((1,), (0,)))
    up = dot(x[...], w_up[...], ((1,), (0,)))
    sig = jax.nn.sigmoid(gate)
    silu = gate * sig
    deriv = up * sig * (1.0 + gate * (1.0 - sig))
    keep = (silu * up).astype(BF16)
    pack = x.shape[0] // capacity
    for i in range(pack):
        part = slice(i * capacity, (i + 1) * capacity)
        place = ((info[0] ^ i) & (pack - 1)) * capacity
        spot = pl.ds(pl.multiple_of(place, capacity), capacity)
        hidden[spot, :] = keep[part]
        slope[spot, :] = deriv[part]
        swish[spot, :] = silu[part]


def mid_kernel(lanes, first, slope, swish, w_gate, w_up, w_down, *refs):
    pieces, (d_gate, d_up), outs = refs[:lanes], refs[lanes : lanes + 2], refs[lanes + 2 :]
    rows, cols = pieces[0].shape
    lane = lax.axis_index("tp")
    part = slice(first, first + rows)
    total = None
    for j in range(lanes):
        term = dot(pieces[j][...], lane_columns(w_down, lane ^ j, cols), ((1,), (1,)))
        total = term if total is None else total + term
    gate = (total * slope[part, :]).astype(BF16)
    up = (total * swish[part, :]).astype(BF16)
    d_gate[...] = gate
    d_up[...] = up
    for j in range(lanes):
        spot = pl.ds(pl.multiple_of((lane ^ j) * cols, cols), cols)
        out = dot(gate, w_gate[spot, :], ((1,), (1,))) + dot(up, w_up[spot, :], ((1,), (1,)))
        outs[j][...] = out.astype(BF16)


def down_kernel(lanes, count, hidden, *refs):
    pieces, out = refs[:-1], refs[-1]
    cols = out.shape[1] // lanes
    lane = lax.axis_index("tp")
    for j in range(lanes):
        total = None
        start = 0
        for g in range(count):
            piece = pieces[g * lanes + j]
            size = piece.shape[0]
            term = dot(hidden[start : start + size], piece[...], ((0,), (0,)))
            total = term if total is None else total + term
            start += size
        spot = pl.ds(pl.multiple_of((lane ^ j) * cols, cols), cols)
        out[:, spot] = total.astype(BF16)


def gate_up_kernel(capacity, count, direct, x, *refs):
    grads, (out_gate, out_up) = refs[: 2 * count], refs[2 * count :]
    order, _, _ = position(direct)
    gates, ups = None, None
    k = 0
    for g in range(count):
        gate, up = grads[2 * g], grads[2 * g + 1]
        for i in range(gate.shape[0] // capacity):
            spot = pl.ds(pl.multiple_of((order ^ k) * capacity, capacity), capacity)
            part = slice(i * capacity, (i + 1) * capacity)
            rows = x[spot, :]
            one = dot(rows, gate[part], ((0,), (0,)))
            two = dot(rows, up[part], ((0,), (0,)))
            gates = one if gates is None else gates + one
            ups = two if ups is None else ups + two
            k += 1
    out_gate[...] = gates.astype(BF16)
    out_up[...] = ups.astype(BF16)


def combine_kernel(select, cot, *refs):
    blocks, (out, kept) = refs[:-2], refs[-2:]
    total = cot[...].astype(F32)
    start = 0
    for block in blocks:
        size = block.shape[0]
        total = total + dot(select[:, start : start + size], block[...], ((1,), (0,)))
        start += size
    out[...] = total.astype(BF16)
    kept[...] = total.astype(BF16)


def mixer_kernel(lanes, direct, gate_in, conv_sum, w_out, *refs):
    pieces = refs[:lanes]
    d_gate_in, d_sum = refs[lanes : lanes + 2]
    own, outs, scratch = refs[lanes + 2], refs[lanes + 3 : -1], refs[-1]
    cols = pieces[0].shape[1]
    order, me, lane = position(direct)
    gate = gate_in[...].astype(F32)
    conv = conv_sum[...].astype(F32)
    mixed = (gate * conv).astype(BF16)
    total = None
    for j in range(lanes):
        spot = pl.ds(pl.multiple_of((lane ^ j) * cols, cols), cols)
        piece = pieces[j][...]
        term = dot(piece, w_out[spot, :], ((1,), (0,)))
        total = term if total is None else total + term
        scratch[spot, :] = dot(piece, mixed, ((0,), (0,)))
    d_gate_in[...] = (total * conv).astype(BF16)
    d_sum[...] = total * gate
    size = own.shape[0]
    if direct:
        for k in range(scratch.shape[0] // size):
            part = scratch[pl.ds(pl.multiple_of((order ^ k) * size, size), size), :]
            if k == 0:
                own[...] = part
            else:
                outs[k - 1][...] = part.astype(BF16)
    else:
        own[...] = scratch[pl.ds(pl.multiple_of(me * size, size), size), :]
        outs[0][...] = scratch[...].astype(BF16)


def flat_call(kernel, ins, outs, flops, limit, scratch=(), space=pltpu.VMEM):
    return pl.pallas_call(
        kernel,
        in_specs=[pl.BlockSpec(memory_space=space)] * len(ins),
        out_specs=[pl.BlockSpec(memory_space=pltpu.VMEM)] * len(outs),
        out_shape=outs,
        scratch_shapes=list(scratch),
        compiler_params=pltpu.CompilerParams(vmem_limit_bytes=limit << 20),
        cost_estimate=pl.CostEstimate(
            flops=flops,
            transcendentals=0,
            bytes_accessed=sum(a.size * a.dtype.itemsize for a in [*ins, *outs]),
        ),
    )(*ins)


def struct(shape, dtype):
    return jax.ShapeDtypeStruct(shape, dtype)


def gather_lanes(own, lanes):
    distance = lanes // 2
    have = {0: own}
    while distance >= 1:
        for j in list(have):
            k = j ^ distance
            have[k] = swap(have[j], "tp", distance)
        distance //= 2
    return [have[j] for j in range(lanes)]


def sum_lanes(parts, lanes):
    have = {j: parts[j].astype(F32) for j in range(lanes)}
    distance = 1
    while distance < lanes:
        sent = {j: swap(have[j].astype(BF16), "tp", distance) for j in have if j & distance}
        have = {
            j: have[j] + sent[j ^ distance].astype(F32) for j in have if not j & distance
        }
        distance *= 2
    return have[0].astype(BF16)


def body(
    cotangent,
    route_ids,
    route_weights,
    expert_inputs,
    gate_weight,
    up_weight,
    down_weight,
    out_weight,
    gate_in,
    conv_sum,
    conv_c,
    conv_v,
    conv_taps,
):
    groups = lax.axis_size("sp")
    lanes = lax.axis_size("tp")
    capacity = expert_inputs.shape[1] // groups
    tokens, model_width = cotangent.shape
    cols = model_width // lanes
    units = gate_weight.shape[2]
    slots = groups * capacity
    channels = gate_in.shape[1]
    part_rows = model_width // groups
    if gate_weight.shape[0] != 1 or lanes & (lanes - 1):
        raise ValueError("unsupported mesh")
    direct = groups == 8
    me = lax.axis_index("sp")
    order = me if direct else jnp.zeros_like(me)
    x = expert_inputs[0]
    w_gate, w_up, w_down = gate_weight[0], up_weight[0], down_weight[0]
    members = [[0], [1, 2, 3], [4, 5], [6, 7]] if direct else [list(range(groups))]
    ids, factors = route_ids.T, route_weights.T
    block = struct((capacity, cols), BF16)

    blocks = flat_call(
        functools.partial(dispatch_kernel, groups, direct),
        in_hbm(ids, factors, cotangent),
        [block] * (groups - 1) if direct else [struct((slots, cols), BF16)],
        2 * slots * tokens * cols,
        14,
        scratch=[
            pltpu.VMEM(ids.shape, jnp.int32),
            pltpu.VMEM(ids.shape, F32),
            pltpu.VMEM((tokens, cols), BF16),
            pltpu.SemaphoreType.DMA((3,)),
        ],
        space=pltpu.HBM,
    )
    select, own_cot, *own_pieces = flat_call(
        functools.partial(local_kernel, lanes, groups, capacity, direct),
        in_hbm(ids, factors, cotangent),
        [struct((tokens, slots), BF16), struct((tokens, cols), BF16)]
        + ([block] * lanes if direct else []),
        2 * slots * tokens * cols,
        14,
        scratch=[
            pltpu.VMEM(ids.shape, jnp.int32),
            pltpu.VMEM(ids.shape, F32),
            pltpu.VMEM((tokens, model_width), BF16),
            pltpu.SemaphoreType.DMA((3,)),
        ],
        space=pltpu.HBM,
    )
    pack = min(groups, 4)
    span = pl.BlockSpec((pack * capacity, units), lambda k, info: (k, 0))
    weights = pl.BlockSpec((model_width, units), lambda k, info: (0, 0))
    hidden, slope, swish = pl.pallas_call(
        functools.partial(pre_kernel, capacity),
        grid_spec=pltpu.PrefetchScalarGridSpec(
            num_scalar_prefetch=1,
            grid=(groups // pack,),
            in_specs=[
                pl.BlockSpec(
                    (pack * capacity, model_width), lambda k, info: ((info[0] // pack) ^ k, 0)
                ),
                weights,
                weights,
            ],
            out_specs=[span] * 3,
        ),
        out_shape=[
            struct((slots, units), BF16),
            struct((slots, units), F32),
            struct((slots, units), F32),
        ],
        compiler_params=pltpu.CompilerParams(vmem_limit_bytes=20 << 20),
        cost_estimate=pl.CostEstimate(
            flops=4 * slots * model_width * units,
            transcendentals=slots * units,
            bytes_accessed=12 << 20,
        ),
        name="pre",
    )(order.astype(jnp.int32)[None], *in_hbm(x, w_gate, w_up))

    def arrive(ks):
        if not direct:
            value = blocks[0].reshape(groups, capacity, cols)
            value = lax.all_to_all(value, "sp", split_axis=0, concat_axis=0, tiled=True)
            return gather_lanes(value.reshape(slots, cols), lanes)
        if ks == [0]:
            return own_pieces
        got = [swap(blocks[k - 1], "sp", k) for k in ks]
        return gather_lanes(jnp.concatenate(got, axis=0), lanes)

    arrived = {}
    for g in reversed(range(len(members))):
        arrived[g] = arrive(members[g])

    grads, returned = {}, {}
    for g, ks in enumerate(members):
        rows = len(ks) * capacity
        gate, up, *parts = flat_call(
            functools.partial(mid_kernel, lanes, ks[0] * capacity),
            (slope, swish, w_gate, w_up, w_down, *arrived[g]),
            [struct((rows, units), BF16)] * 2 + [struct((rows, cols), BF16)] * lanes,
            6 * rows * model_width * units,
            14,
        )
        grads[g] = (gate, up)
        total = sum_lanes(parts, lanes)
        if not direct:
            total = total.reshape(groups, capacity, cols)
            total = lax.all_to_all(total, "sp", split_axis=0, concat_axis=0, tiled=True)
            returned[0] = total.reshape(slots, cols)
        else:
            for i, k in enumerate(ks):
                one = total[i * capacity : (i + 1) * capacity]
                returned[k] = swap(one, "sp", k) if k else one

    count = len(members)
    flat = [piece for g in range(count) for piece in arrived[g]]
    (grad_down,) = flat_call(
        functools.partial(down_kernel, lanes, count),
        (hidden, *flat),
        [struct((units, model_width), BF16)],
        2 * slots * model_width * units,
        16,
    )
    flat = [grad for g in range(count) for grad in grads[g]]
    grad_gate, grad_up = flat_call(
        functools.partial(gate_up_kernel, capacity, count, direct),
        (x, *flat),
        [struct((model_width, units), BF16)] * 2,
        4 * slots * model_width * units,
        28,
    )
    grad_input, kept = flat_call(
        combine_kernel,
        (select, own_cot, *[returned[k] for k in sorted(returned)]),
        [struct((tokens, cols), BF16)] * 2,
        2 * slots * tokens * cols,
        16,
    )
    pieces = gather_lanes(kept, lanes)
    part = struct((part_rows, channels), BF16)
    outs = [part] * (groups - 1) if direct else [struct((model_width, channels), BF16)]
    shapes = [
        struct((tokens, channels), BF16),
        struct((tokens, channels), F32),
        struct((part_rows, channels), F32),
    ] + outs
    grad_gate_in, grad_sum, own, *terms = flat_call(
        functools.partial(mixer_kernel, lanes, direct),
        (gate_in, conv_sum, out_weight, *pieces),
        shapes,
        4 * tokens * model_width * channels,
        16,
        scratch=[pltpu.VMEM((model_width, channels), F32)],
    )
    back = [(i, i - 1) for i in range(1, groups)]
    next_rows = lax.ppermute(grad_sum[:2], "sp", back)
    if direct:
        grad_out_weight = own
        for k in range(1, groups):
            term = swap(terms[k - 1], "sp", k)
            grad_out_weight = grad_out_weight + term.astype(F32)
    else:
        value = terms[0].reshape(groups, part_rows, channels)
        value = lax.all_to_all(value, "sp", split_axis=0, concat_axis=0, tiled=True)
        others = (jnp.arange(groups) != me)[:, None, None]
        grad_out_weight = own + jnp.sum(jnp.where(others, value.astype(F32), 0.0), axis=0)
    extended = jnp.concatenate([grad_sum, next_rows], axis=0)
    grad_prod = (
        conv_taps[0] * extended[2:] + conv_taps[1] * extended[1:-1] + conv_taps[2] * extended[:-2]
    )
    grad_conv_c = (grad_prod * conv_v.astype(F32)).astype(BF16)
    grad_conv_v = (grad_prod * conv_c.astype(F32)).astype(BF16)
    return (
        grad_input,
        grad_gate[None],
        grad_up[None],
        grad_down[None],
        grad_out_weight,
        grad_gate_in,
        grad_conv_c,
        grad_conv_v,
    )


def solution(mesh):
    placed = (
        P("sp", None),
        P("sp", None),
        P("sp", None),
        P("sp", None, None),
        P("sp", None, "tp"),
        P("sp", None, "tp"),
        P("sp", "tp", None),
        P(None, "tp"),
        P("sp", "tp"),
        P("sp", "tp"),
        P("sp", "tp"),
        P("sp", "tp"),
        P(None, "tp"),
    )
    return jax.shard_map(
        body,
        mesh=mesh,
        in_specs=placed,
        out_specs=(
            P("sp", "tp"),
            P("sp", None, "tp"),
            P("sp", None, "tp"),
            P("sp", "tp", None),
            P("sp", "tp"),
            P("sp", "tp"),
            P("sp", "tp"),
            P("sp", "tp"),
        ),
        check_vma=False,
    )
```

```python
import functools
import math

import jax
import jax.numpy as jnp
from jax import lax
from jax.experimental import pallas as pl
from jax.experimental.pallas import tpu as pltpu
from jax.sharding import PartitionSpec as P


F32 = jnp.float32
BF16 = jnp.bfloat16


def dot(a, b, contract):
    return lax.dot_general(a, b, (contract, ((), ())), preferred_element_type=F32)


def swap(value, axis, distance):
    route = [(i, i ^ distance) for i in range(lax.axis_size(axis))]
    return lax.ppermute(value, axis, route)


def position(direct):
    me = lax.axis_index("sp")
    return (me if direct else 0), me, lax.axis_index("tp")


def routing(ids, weights, experts, capacity, order):
    tokens = ids.shape[1]
    slots = experts * capacity
    labels = ids[...] ^ order
    expert = lax.broadcasted_iota(jnp.int32, (experts, tokens), 0)
    hit = jnp.zeros((experts, tokens), F32)
    factor = jnp.zeros((experts, tokens), F32)
    for k in range(labels.shape[0]):
        same = expert == labels[k : k + 1]
        hit = hit + same.astype(F32)
        factor = factor + jnp.where(same, weights[k : k + 1], 0.0)
    earlier = (
        lax.broadcasted_iota(jnp.int32, (tokens, tokens), 0)
        < lax.broadcasted_iota(jnp.int32, (tokens, tokens), 1)
    ).astype(F32)
    before = dot(hit.astype(BF16), earlier.astype(BF16), ((1,), (0,))).astype(jnp.int32)
    rank = jnp.where(hit > 0, before, -1)
    row = lax.broadcasted_iota(jnp.int32, (experts, capacity, tokens), 1)
    chosen = (rank[:, None, :] == row).astype(F32)
    scale = jnp.sum(chosen * factor[:, None, :], axis=2, keepdims=True).reshape(slots, 1)
    return chosen.reshape(slots, tokens), scale


def lane_columns_of(ref, lane, cols):
    return ref.at[:, pl.ds(pl.multiple_of(lane * cols, cols), cols)]


def in_hbm(*arrays):
    return [pltpu.with_memory_space_constraint(a, pltpu.HBM) for a in arrays]


def lane_columns(ref, lane, cols):
    return ref[:, pl.ds(pl.multiple_of(lane * cols, cols), cols)]


def dispatch_kernel(experts, direct, ids_in, weights_in, cot_in, *refs):
    blocks, (ids, weights, cot, sems) = refs[:-4], refs[-4:]
    order, _, lane = position(direct)
    capacity = blocks[-1].shape[0] if direct else blocks[0].shape[0] // experts
    cols = cot.shape[1]
    copies = [
        pltpu.make_async_copy(ids_in, ids, sems.at[0]),
        pltpu.make_async_copy(weights_in, weights, sems.at[1]),
        pltpu.make_async_copy(lane_columns_of(cot_in, lane, cols), cot, sems.at[2]),
    ]
    for copy in copies:
        copy.start()
    copies[0].wait()
    copies[1].wait()
    chosen, scale = routing(ids, weights, experts, capacity, order)
    chosen = chosen.astype(BF16)
    copies[2].wait()
    if direct:
        rows = (dot(chosen[capacity:], cot[...], ((1,), (0,))) * scale[capacity:]).astype(BF16)
        for k in range(1, experts):
            blocks[k - 1][...] = rows[(k - 1) * capacity : k * capacity]
    else:
        blocks[0][...] = (dot(chosen, cot[...], ((1,), (0,))) * scale).astype(BF16)


def local_kernel(lanes, experts, capacity, direct, ids_in, weights_in, cot_in, *refs):
    sources, targets = refs[:3], refs[3:6]
    select, own_cot, *pieces = refs[6:-4]
    ids, weights, cot, sems = refs[-4:]
    order, _, lane = position(direct)
    cols = cot.shape[1] // lanes
    copies = [
        pltpu.make_async_copy(ids_in, ids, sems.at[0]),
        pltpu.make_async_copy(weights_in, weights, sems.at[1]),
        pltpu.make_async_copy(cot_in, cot, sems.at[2]),
    ]
    moves = [pltpu.make_async_copy(u, v, sems.at[3 + i]) for i, (u, v) in enumerate(zip(sources, targets))]
    for copy in copies + moves:
        copy.start()
    for copy in copies:
        copy.wait()
    chosen, scale = routing(ids, weights, experts, capacity, order)
    select[...] = chosen.T.astype(BF16)
    own_cot[...] = lane_columns(cot, lane, cols)
    if direct:
        first = chosen[:capacity].astype(BF16)
        for j in range(lanes):
            rows = dot(first, lane_columns(cot, lane ^ j, cols), ((1,), (0,)))
            pieces[j][...] = (rows * scale[:capacity]).astype(BF16)
    for move in moves:
        move.wait()


def pre_kernel(capacity, half, direct, x_in, w_gate, w_up, hidden, slope, swish, x, sem):
    order, _, _ = position(direct)
    rows = x.shape[0]
    pack = rows // capacity
    start = pl.multiple_of(((order // pack) ^ half) * rows, rows)
    copy = pltpu.make_async_copy(x_in.at[pl.ds(start, rows)], x, sem.at[0])
    copy.start()
    copy.wait()
    gate = dot(x[...], w_gate[...], ((1,), (0,)))
    up = dot(x[...], w_up[...], ((1,), (0,)))
    sig = jax.nn.sigmoid(gate)
    silu = gate * sig
    deriv = up * sig * (1.0 + gate * (1.0 - sig))
    keep = (silu * up).astype(BF16)
    for i in range(pack):
        part = slice(i * capacity, (i + 1) * capacity)
        place = ((order ^ i) & (pack - 1)) * capacity
        spot = pl.ds(pl.multiple_of(place, capacity), capacity)
        hidden[spot, :] = keep[part]
        slope[spot, :] = deriv[part]
        swish[spot, :] = silu[part]


def mid_kernel(lanes, first, slope, swish, w_gate, w_up, w_down, *refs):
    pieces, (d_gate, d_up), outs = refs[:lanes], refs[lanes : lanes + 2], refs[lanes + 2 :]
    rows, cols = pieces[0].shape
    lane = lax.axis_index("tp")
    part = slice(first, first + rows)
    total = None
    for j in range(lanes):
        term = dot(pieces[j][...], lane_columns(w_down, lane ^ j, cols), ((1,), (1,)))
        total = term if total is None else total + term
    gate = (total * slope[part, :]).astype(BF16)
    up = (total * swish[part, :]).astype(BF16)
    d_gate[...] = gate
    d_up[...] = up
    for j in range(lanes):
        spot = pl.ds(pl.multiple_of((lane ^ j) * cols, cols), cols)
        out = dot(gate, w_gate[spot, :], ((1,), (1,))) + dot(up, w_up[spot, :], ((1,), (1,)))
        outs[j][...] = out.astype(BF16)


def down_kernel(lanes, places, *refs):
    count = 1 + max(which for which, _ in places)
    hidden, pieces, out = refs[:count], refs[count:-1], refs[-1]
    cols = out.shape[1] // lanes
    lane = lax.axis_index("tp")
    for j in range(lanes):
        total = None
        for g, (which, start) in enumerate(places):
            piece = pieces[g * lanes + j]
            rows = hidden[which][start : start + piece.shape[0]]
            term = dot(rows, piece[...], ((0,), (0,)))
            total = term if total is None else total + term
        spot = pl.ds(pl.multiple_of((lane ^ j) * cols, cols), cols)
        out[:, spot] = total.astype(BF16)


def conv_kernel(d_sum, following, taps, conv_v, conv_c, d_conv_c, d_conv_v):
    value = d_sum[...]
    last = value.shape[0] - 1
    row = lax.broadcasted_iota(jnp.int32, value.shape, 0)
    once = jnp.where(row == last, following[0:1], pltpu.roll(value, last, 0))
    twice = jnp.where(row == last, following[1:2], pltpu.roll(once, last, 0))
    total = taps[0:1] * twice + taps[1:2] * once + taps[2:3] * value
    d_conv_c[...] = (total * conv_v[...].astype(F32)).astype(BF16)
    d_conv_v[...] = (total * conv_c[...].astype(F32)).astype(BF16)


def in_vmem(array):
    return pltpu.VMEM(array.shape, array.dtype)


def gate_up_kernel(capacity, members, direct, x, *refs):
    grads, (out_gate, out_up) = refs[:-2], refs[-2:]
    order, _, _ = position(direct)
    gates, ups = None, None
    for g, ks in enumerate(members):
        gate, up = grads[2 * g], grads[2 * g + 1]
        for i, k in enumerate(ks):
            spot = pl.ds(pl.multiple_of((order ^ k) * capacity, capacity), capacity)
            part = slice(i * capacity, (i + 1) * capacity)
            rows = x[spot, :]
            one = dot(rows, gate[part], ((0,), (0,)))
            two = dot(rows, up[part], ((0,), (0,)))
            gates = one if gates is None else gates + one
            ups = two if ups is None else ups + two
    out_gate[...] = gates.astype(BF16)
    out_up[...] = ups.astype(BF16)


def combine_kernel(select, cot, *refs):
    blocks, (out, kept) = refs[:-2], refs[-2:]
    total = cot[...].astype(F32)
    start = 0
    for block in blocks:
        size = block.shape[0]
        total = total + dot(select[:, start : start + size], block[...], ((1,), (0,)))
        start += size
    out[...] = total.astype(BF16)
    kept[...] = total.astype(BF16)


def mixer_kernel(lanes, direct, gate_in, conv_sum, w_out, *refs):
    pieces = refs[:lanes]
    d_gate_in, d_sum = refs[lanes : lanes + 2]
    own, outs, scratch = refs[lanes + 2], refs[lanes + 3 : -1], refs[-1]
    cols = pieces[0].shape[1]
    order, me, lane = position(direct)
    gate = gate_in[...].astype(F32)
    conv = conv_sum[...].astype(F32)
    mixed = (gate * conv).astype(BF16)
    total = None
    for j in range(lanes):
        spot = pl.ds(pl.multiple_of((lane ^ j) * cols, cols), cols)
        piece = pieces[j][...]
        term = dot(piece, w_out[spot, :], ((1,), (0,)))
        total = term if total is None else total + term
        scratch[spot, :] = dot(piece, mixed, ((0,), (0,)))
    d_gate_in[...] = (total * conv).astype(BF16)
    d_sum[...] = total * gate
    size = own.shape[0]
    if direct:

        def part(k):
            return scratch[pl.ds(pl.multiple_of((order ^ k) * size, size), size), :]

        own[...] = part(0)
        near, stay, cross = outs[:3], outs[3], outs[4]
        for k in (1, 2, 3):
            near[k - 1][...] = part(k).astype(BF16)
        for i, k in enumerate((4, 6)):
            spot = slice(i * size, (i + 1) * size)
            stay[spot] = part(k).astype(BF16)
            cross[spot] = part(k ^ 1).astype(BF16)
    else:
        own[...] = scratch[pl.ds(pl.multiple_of(me * size, size), size), :]
        outs[0][...] = scratch[...].astype(BF16)


def flat_call(kernel, ins, outs, flops, limit, scratch=(), space=pltpu.VMEM):
    return pl.pallas_call(
        kernel,
        in_specs=[
            pl.BlockSpec(memory_space=space[i] if isinstance(space, tuple) else space)
            for i in range(len(ins))
        ],
        out_specs=[pl.BlockSpec(memory_space=pltpu.VMEM)] * len(outs),
        out_shape=outs,
        scratch_shapes=list(scratch),
        compiler_params=pltpu.CompilerParams(vmem_limit_bytes=limit << 20),
        cost_estimate=pl.CostEstimate(
            flops=flops,
            transcendentals=0,
            bytes_accessed=sum(math.prod(a.shape) * a.dtype.itemsize for a in [*ins, *outs]),
        ),
    )(*ins)


def struct(shape, dtype):
    return jax.ShapeDtypeStruct(shape, dtype)


def spread(have, lanes, distance):
    while distance >= 1:
        for j in list(have):
            k = j ^ distance
            have[k] = swap(have[j], "tp", distance)
        distance //= 2
    return [have[j] for j in range(lanes)]


def gather_lanes(own, lanes):
    return spread({0: own}, lanes, lanes // 2)


def sum_lanes(parts, lanes):
    have = {j: parts[j].astype(F32) for j in range(lanes)}
    distance = 1
    while distance < lanes:
        sent = {j: swap(have[j].astype(BF16), "tp", distance) for j in have if j & distance}
        have = {
            j: have[j] + sent[j ^ distance].astype(F32) for j in have if not j & distance
        }
        distance *= 2
    return have[0].astype(BF16)


def body(
    cotangent,
    route_ids,
    route_weights,
    expert_inputs,
    gate_weight,
    up_weight,
    down_weight,
    out_weight,
    gate_in,
    conv_sum,
    conv_c,
    conv_v,
    conv_taps,
):
    groups = lax.axis_size("sp")
    lanes = lax.axis_size("tp")
    capacity = expert_inputs.shape[1] // groups
    tokens, model_width = cotangent.shape
    cols = model_width // lanes
    units = gate_weight.shape[2]
    slots = groups * capacity
    channels = gate_in.shape[1]
    part_rows = model_width // groups
    if gate_weight.shape[0] != 1 or lanes & (lanes - 1):
        raise ValueError("unsupported mesh")
    direct = groups == 8
    me = lax.axis_index("sp")
    x = expert_inputs[0]
    w_gate, w_up, w_down = gate_weight[0], up_weight[0], down_weight[0]
    members = [[0], [1, 2, 3], [4, 5], [6, 7]] if direct else [list(range(groups))]
    ids, factors = route_ids.T, route_weights.T
    block = struct((capacity, cols), BF16)

    blocks = flat_call(
        functools.partial(dispatch_kernel, groups, direct),
        in_hbm(ids, factors, cotangent),
        [block] * (groups - 1) if direct else [struct((slots, cols), BF16)],
        2 * slots * tokens * cols,
        14,
        scratch=[
            pltpu.VMEM(ids.shape, jnp.int32),
            pltpu.VMEM(ids.shape, F32),
            pltpu.VMEM((tokens, cols), BF16),
            pltpu.SemaphoreType.DMA((3,)),
        ],
        space=pltpu.HBM,
    )
    w_gate, w_up, w_down, select, own_cot, *own_pieces = flat_call(
        functools.partial(local_kernel, lanes, groups, capacity, direct),
        in_hbm(ids, factors, cotangent, w_gate, w_up, w_down),
        [in_vmem(w) for w in (w_gate, w_up, w_down)]
        + [struct((tokens, slots), BF16), struct((tokens, cols), BF16)]
        + ([block] * lanes if direct else []),
        2 * slots * tokens * cols,
        14,
        scratch=[
            pltpu.VMEM(ids.shape, jnp.int32),
            pltpu.VMEM(ids.shape, F32),
            pltpu.VMEM((tokens, model_width), BF16),
            pltpu.SemaphoreType.DMA((6,)),
        ],
        space=pltpu.HBM,
    )
    half_slots = slots // 2
    halves = [
        flat_call(
            functools.partial(pre_kernel, capacity, h, direct),
            (*in_hbm(x), w_gate, w_up),
            [struct((half_slots, units), t) for t in (BF16, F32, F32)],
            4 * half_slots * model_width * units,
            12,
            scratch=[pltpu.VMEM((half_slots, model_width), BF16), pltpu.SemaphoreType.DMA((1,))],
            space=(pltpu.HBM, pltpu.VMEM, pltpu.VMEM),
        )
        for h in range(2)
    ]

    def arrive(ks):
        if not direct:
            value = blocks[0].reshape(groups, capacity, cols)
            value = lax.all_to_all(value, "sp", split_axis=0, concat_axis=0, tiled=True)
            return gather_lanes(value.reshape(slots, cols), lanes)
        if ks == [0]:
            return own_pieces
        got = [swap(blocks[k - 1], "sp", k) for k in ks]
        return gather_lanes(jnp.concatenate(got, axis=0), lanes)

    arrived = {}
    for g in reversed(range(len(members))):
        arrived[g] = arrive(members[g])

    grads, returned = {}, {}
    for g, ks in enumerate(members):
        rows = len(ks) * capacity
        which, offset = divmod(ks[0] * capacity, half_slots)
        _, slope, swish = halves[which]
        if not direct:
            slope, swish = (jnp.concatenate([h[i] for h in halves]) for i in (1, 2))
        gate, up, *parts = flat_call(
            functools.partial(mid_kernel, lanes, offset),
            (slope, swish, w_gate, w_up, w_down, *arrived[g]),
            [struct((rows, units), BF16)] * 2 + [struct((rows, cols), BF16)] * lanes,
            6 * rows * model_width * units,
            14,
        )
        grads[g] = (gate, up)
        total = sum_lanes(parts, lanes)
        if not direct:
            total = total.reshape(groups, capacity, cols)
            total = lax.all_to_all(total, "sp", split_axis=0, concat_axis=0, tiled=True)
            returned[0] = total.reshape(slots, cols)
        else:
            for i, k in enumerate(ks):
                one = total[i * capacity : (i + 1) * capacity]
                returned[k] = swap(one, "sp", k) if k else one

    count = len(members)
    places = [divmod(ks[0] * capacity, half_slots) for ks in members]
    hidden = [h[0] for h in halves] if direct else [jnp.concatenate([h[0] for h in halves])]
    flat = [piece for g in range(count) for piece in arrived[g]]
    (grad_down,) = flat_call(
        functools.partial(down_kernel, lanes, places),
        (*hidden, *flat),
        [struct((units, model_width), BF16)],
        2 * slots * model_width * units,
        16,
    )
    flat = [grad for g in range(count) for grad in grads[g]]
    grad_gate, grad_up = flat_call(
        functools.partial(gate_up_kernel, capacity, members, direct),
        (x, *flat),
        [struct((model_width, units), BF16)] * 2,
        4 * slots * model_width * units,
        28,
    )
    grad_input, kept = flat_call(
        combine_kernel,
        (select, own_cot, *[returned[k] for k in sorted(returned)]),
        [struct((tokens, cols), BF16)] * 2,
        2 * slots * tokens * cols,
        16,
    )
    pieces = gather_lanes(kept, lanes)
    part = struct((part_rows, channels), BF16)
    pair = struct((2 * part_rows, channels), BF16)
    outs = [part] * 3 + [pair] * 2 if direct else [struct((model_width, channels), BF16)]
    shapes = [
        struct((tokens, channels), BF16),
        struct((tokens, channels), F32),
        struct((part_rows, channels), F32),
    ] + outs
    grad_gate_in, grad_sum, own, *terms = flat_call(
        functools.partial(mixer_kernel, lanes, direct),
        (gate_in, conv_sum, out_weight, *pieces),
        shapes,
        4 * tokens * model_width * channels,
        16,
        scratch=[pltpu.VMEM((model_width, channels), F32)],
    )
    back = [(i, i - 1) for i in range(1, groups)]
    next_rows = lax.ppermute(grad_sum[:2], "sp", back)
    if direct:
        arrived_terms = [swap(terms[k - 1], "sp", k) for k in (1, 2, 3)]
        crossed = swap(terms[4], "sp", 1)
        stay = (terms[3].astype(F32) + crossed.astype(F32)).astype(BF16)
        for i, k in enumerate((4, 6)):
            half = stay[i * part_rows : (i + 1) * part_rows]
            arrived_terms.append(swap(half, "sp", k))
        grad_out_weight = own
        for term in arrived_terms:
            grad_out_weight = grad_out_weight + term.astype(F32)
    else:
        value = terms[0].reshape(groups, part_rows, channels)
        value = lax.all_to_all(value, "sp", split_axis=0, concat_axis=0, tiled=True)
        others = (jnp.arange(groups) != me)[:, None, None]
        grad_out_weight = own + jnp.sum(jnp.where(others, value.astype(F32), 0.0), axis=0)
    grad_conv_c, grad_conv_v = flat_call(
        conv_kernel,
        (grad_sum, next_rows, conv_taps, conv_v, conv_c),
        [struct((tokens, channels), BF16)] * 2,
        8 * tokens * channels,
        8,
    )
    return (
        grad_input,
        grad_gate[None],
        grad_up[None],
        grad_down[None],
        grad_out_weight,
        grad_gate_in,
        grad_conv_c,
        grad_conv_v,
    )


def solution(mesh):
    placed = (
        P("sp", None),
        P("sp", None),
        P("sp", None),
        P("sp", None, None),
        P("sp", None, "tp"),
        P("sp", None, "tp"),
        P("sp", "tp", None),
        P(None, "tp"),
        P("sp", "tp"),
        P("sp", "tp"),
        P("sp", "tp"),
        P("sp", "tp"),
        P(None, "tp"),
    )
    return jax.shard_map(
        body,
        mesh=mesh,
        in_specs=placed,
        out_specs=(
            P("sp", "tp"),
            P("sp", None, "tp"),
            P("sp", None, "tp"),
            P("sp", "tp", None),
            P("sp", "tp"),
            P("sp", "tp"),
            P("sp", "tp"),
            P("sp", "tp"),
        ),
        check_vma=False,
    )
```

```python
import functools
import math

import jax
import jax.numpy as jnp
from jax import lax
from jax.experimental import pallas as pl
from jax.experimental.pallas import tpu as pltpu
from jax.sharding import PartitionSpec as P


F32 = jnp.float32
BF16 = jnp.bfloat16


def dot(a, b, contract):
    return lax.dot_general(a, b, (contract, ((), ())), preferred_element_type=F32)


def swap(value, axis, distance):
    route = [(i, i ^ distance) for i in range(lax.axis_size(axis))]
    return lax.ppermute(value, axis, route)


def position(direct):
    me = lax.axis_index("sp")
    return (me if direct else 0), me, lax.axis_index("tp")


def routing(ids, weights, experts, capacity, order):
    tokens = ids.shape[1]
    slots = experts * capacity
    labels = ids[...] ^ order
    expert = lax.broadcasted_iota(jnp.int32, (experts, tokens), 0)
    hit = jnp.zeros((experts, tokens), F32)
    factor = jnp.zeros((experts, tokens), F32)
    for k in range(labels.shape[0]):
        same = expert == labels[k : k + 1]
        hit = hit + same.astype(F32)
        factor = factor + jnp.where(same, weights[k : k + 1], 0.0)
    earlier = (
        lax.broadcasted_iota(jnp.int32, (tokens, tokens), 0)
        < lax.broadcasted_iota(jnp.int32, (tokens, tokens), 1)
    ).astype(F32)
    before = dot(hit.astype(BF16), earlier.astype(BF16), ((1,), (0,))).astype(jnp.int32)
    rank = jnp.where(hit > 0, before, -1)
    row = lax.broadcasted_iota(jnp.int32, (experts, capacity, tokens), 1)
    chosen = (rank[:, None, :] == row).astype(F32)
    scale = jnp.sum(chosen * factor[:, None, :], axis=2, keepdims=True).reshape(slots, 1)
    return chosen.reshape(slots, tokens), scale


def lane_columns_of(ref, lane, cols):
    return ref.at[:, pl.ds(pl.multiple_of(lane * cols, cols), cols)]


def in_hbm(*arrays):
    return [pltpu.with_memory_space_constraint(a, pltpu.HBM) for a in arrays]


def lane_columns(ref, lane, cols):
    return ref[:, pl.ds(pl.multiple_of(lane * cols, cols), cols)]


def dispatch_kernel(experts, direct, ids_in, weights_in, cot_in, *refs):
    blocks, (ids, weights, cot, sems) = refs[:-4], refs[-4:]
    order, _, lane = position(direct)
    capacity = blocks[-1].shape[0] if direct else blocks[0].shape[0] // experts
    cols = cot.shape[1]
    copies = [
        pltpu.make_async_copy(ids_in, ids, sems.at[0]),
        pltpu.make_async_copy(weights_in, weights, sems.at[1]),
        pltpu.make_async_copy(lane_columns_of(cot_in, lane, cols), cot, sems.at[2]),
    ]
    for copy in copies:
        copy.start()
    copies[0].wait()
    copies[1].wait()
    chosen, scale = routing(ids, weights, experts, capacity, order)
    chosen = chosen.astype(BF16)
    copies[2].wait()
    if direct:
        rows = (dot(chosen[capacity:], cot[...], ((1,), (0,))) * scale[capacity:]).astype(BF16)
        for k in range(1, experts):
            blocks[k - 1][...] = rows[(k - 1) * capacity : k * capacity]
    else:
        blocks[0][...] = (dot(chosen, cot[...], ((1,), (0,))) * scale).astype(BF16)


def local_kernel(lanes, experts, capacity, direct, ids_in, weights_in, cot_in, *refs):
    sources, targets = refs[:3], refs[3:6]
    select, own_cot, *pieces = refs[6:-4]
    ids, weights, cot, sems = refs[-4:]
    order, _, lane = position(direct)
    cols = cot.shape[1] // lanes
    copies = [
        pltpu.make_async_copy(ids_in, ids, sems.at[0]),
        pltpu.make_async_copy(weights_in, weights, sems.at[1]),
        pltpu.make_async_copy(cot_in, cot, sems.at[2]),
    ]
    moves = [pltpu.make_async_copy(u, v, sems.at[3 + i]) for i, (u, v) in enumerate(zip(sources, targets))]
    for copy in copies + moves:
        copy.start()
    for copy in copies:
        copy.wait()
    chosen, scale = routing(ids, weights, experts, capacity, order)
    select[...] = chosen.T.astype(BF16)
    own_cot[...] = lane_columns(cot, lane, cols)
    if direct:
        first = chosen[:capacity].astype(BF16)
        for j in range(lanes):
            rows = dot(first, lane_columns(cot, lane ^ j, cols), ((1,), (0,)))
            pieces[j][...] = (rows * scale[:capacity]).astype(BF16)
    for move in moves:
        move.wait()


def pre_kernel(capacity, half, direct, x_in, w_gate, w_up, hidden, slope, swish, x, sem):
    order, _, _ = position(direct)
    rows = x.shape[0]
    pack = rows // capacity
    start = pl.multiple_of(((order // pack) ^ half) * rows, rows)
    copy = pltpu.make_async_copy(x_in.at[pl.ds(start, rows)], x, sem.at[0])
    copy.start()
    copy.wait()
    gate = dot(x[...], w_gate[...], ((1,), (0,)))
    up = dot(x[...], w_up[...], ((1,), (0,)))
    sig = jax.nn.sigmoid(gate)
    silu = gate * sig
    deriv = up * sig * (1.0 + gate * (1.0 - sig))
    keep = (silu * up).astype(BF16)
    for i in range(pack):
        part = slice(i * capacity, (i + 1) * capacity)
        place = ((order ^ i) & (pack - 1)) * capacity
        spot = pl.ds(pl.multiple_of(place, capacity), capacity)
        hidden[spot, :] = keep[part]
        slope[spot, :] = deriv[part]
        swish[spot, :] = silu[part]


def mid_kernel(lanes, first, slope, swish, w_gate, w_up, w_down, *refs):
    pieces, (d_gate, d_up), outs = refs[:lanes], refs[lanes : lanes + 2], refs[lanes + 2 :]
    rows, cols = pieces[0].shape
    lane = lax.axis_index("tp")
    part = slice(first, first + rows)
    total = None
    for j in range(lanes):
        term = dot(pieces[j][...], lane_columns(w_down, lane ^ j, cols), ((1,), (1,)))
        total = term if total is None else total + term
    gate = (total * slope[part, :]).astype(BF16)
    up = (total * swish[part, :]).astype(BF16)
    d_gate[...] = gate
    d_up[...] = up
    for j in range(lanes):
        spot = pl.ds(pl.multiple_of((lane ^ j) * cols, cols), cols)
        out = dot(gate, w_gate[spot, :], ((1,), (1,))) + dot(up, w_up[spot, :], ((1,), (1,)))
        outs[j][...] = out.astype(BF16)


def down_kernel(lanes, places, *refs):
    count = 1 + max(which for which, _ in places)
    hidden, pieces, out = refs[:count], refs[count:-1], refs[-1]
    cols = out.shape[1] // lanes
    lane = lax.axis_index("tp")
    for j in range(lanes):
        total = None
        for g, (which, start) in enumerate(places):
            piece = pieces[g * lanes + j]
            rows = hidden[which][start : start + piece.shape[0]]
            term = dot(rows, piece[...], ((0,), (0,)))
            total = term if total is None else total + term
        spot = pl.ds(pl.multiple_of((lane ^ j) * cols, cols), cols)
        out[:, spot] = total.astype(BF16)


def conv_kernel(d_sum, following, taps, conv_v, conv_c, d_conv_c, d_conv_v):
    value = d_sum[...]
    last = value.shape[0] - 1
    row = lax.broadcasted_iota(jnp.int32, value.shape, 0)
    once = jnp.where(row == last, following[0:1], pltpu.roll(value, last, 0))
    twice = jnp.where(row == last, following[1:2], pltpu.roll(once, last, 0))
    total = taps[0:1] * twice + taps[1:2] * once + taps[2:3] * value
    d_conv_c[...] = (total * conv_v[...].astype(F32)).astype(BF16)
    d_conv_v[...] = (total * conv_c[...].astype(F32)).astype(BF16)


def in_vmem(array):
    return pltpu.VMEM(array.shape, array.dtype)


def gate_up_kernel(capacity, members, direct, x, *refs):
    grads, (out_gate, out_up) = refs[:-2], refs[-2:]
    order, _, _ = position(direct)
    gates, ups = {}, {}
    for g, ks in enumerate(members):
        for i, k in enumerate(ks):
            part = slice(i * capacity, (i + 1) * capacity)
            gates[k] = grads[2 * g][part]
            ups[k] = grads[2 * g + 1][part]

    def paired(values, k):
        low, high = values[k], values[k + 1]
        if not direct:
            return jnp.concatenate([low, high], axis=0)
        odd = (order & 1) == 1
        return jnp.concatenate([jnp.where(odd, high, low), jnp.where(odd, low, high)], axis=0)

    for values, out in ((gates, out_gate), (ups, out_up)):
        total = None
        for k in range(0, len(values), 2):
            start = pl.multiple_of(((order // 2) ^ (k // 2)) * 2 * capacity, 2 * capacity)
            term = dot(x[pl.ds(start, 2 * capacity), :], paired(values, k), ((0,), (0,)))
            total = term if total is None else total + term
        out[...] = total.astype(BF16)


def combine_kernel(select, cot, *refs):
    blocks, (out, kept) = refs[:-2], refs[-2:]
    total = cot[...].astype(F32)
    start = 0
    for block in blocks:
        size = block.shape[0]
        total = total + dot(select[:, start : start + size], block[...], ((1,), (0,)))
        start += size
    out[...] = total.astype(BF16)
    kept[...] = total.astype(BF16)


def mixer_kernel(lanes, direct, gate_in, conv_sum, w_out, *refs):
    pieces = refs[:lanes]
    d_gate_in, d_sum = refs[lanes : lanes + 2]
    own, outs, scratch = refs[lanes + 2], refs[lanes + 3 : -1], refs[-1]
    cols = pieces[0].shape[1]
    order, me, lane = position(direct)
    gate = gate_in[...].astype(F32)
    conv = conv_sum[...].astype(F32)
    mixed = (gate * conv).astype(BF16)
    total = None
    for j in range(lanes):
        spot = pl.ds(pl.multiple_of((lane ^ j) * cols, cols), cols)
        piece = pieces[j][...]
        term = dot(piece, w_out[spot, :], ((1,), (0,)))
        total = term if total is None else total + term
        scratch[spot, :] = dot(piece, mixed, ((0,), (0,)))
    d_gate_in[...] = (total * conv).astype(BF16)
    d_sum[...] = total * gate
    size = own.shape[0]
    if direct:

        def part(k):
            return scratch[pl.ds(pl.multiple_of((order ^ k) * size, size), size), :]

        own[...] = part(0)
        near, stay, cross = outs[:3], outs[3], outs[4]
        for k in (1, 2, 3):
            near[k - 1][...] = part(k).astype(BF16)
        for i, k in enumerate((4, 6)):
            spot = slice(i * size, (i + 1) * size)
            stay[spot] = part(k).astype(BF16)
            cross[spot] = part(k ^ 1).astype(BF16)
    else:
        own[...] = scratch[pl.ds(pl.multiple_of(me * size, size), size), :]
        outs[0][...] = scratch[...].astype(BF16)


def flat_call(kernel, ins, outs, flops, limit, scratch=(), space=pltpu.VMEM):
    return pl.pallas_call(
        kernel,
        in_specs=[
            pl.BlockSpec(memory_space=space[i] if isinstance(space, tuple) else space)
            for i in range(len(ins))
        ],
        out_specs=[pl.BlockSpec(memory_space=pltpu.VMEM)] * len(outs),
        out_shape=outs,
        scratch_shapes=list(scratch),
        compiler_params=pltpu.CompilerParams(vmem_limit_bytes=limit << 20),
        cost_estimate=pl.CostEstimate(
            flops=flops,
            transcendentals=0,
            bytes_accessed=sum(math.prod(a.shape) * a.dtype.itemsize for a in [*ins, *outs]),
        ),
    )(*ins)


def struct(shape, dtype):
    return jax.ShapeDtypeStruct(shape, dtype)


def spread(have, lanes, distance):
    while distance >= 1:
        for j in list(have):
            k = j ^ distance
            have[k] = swap(have[j], "tp", distance)
        distance //= 2
    return [have[j] for j in range(lanes)]


def gather_lanes(own, lanes):
    return spread({0: own}, lanes, lanes // 2)


def sum_lanes(parts, lanes):
    have = {j: parts[j].astype(F32) for j in range(lanes)}
    distance = 1
    while distance < lanes:
        sent = {j: swap(have[j].astype(BF16), "tp", distance) for j in have if j & distance}
        have = {
            j: have[j] + sent[j ^ distance].astype(F32) for j in have if not j & distance
        }
        distance *= 2
    return have[0].astype(BF16)


def body(
    cotangent,
    route_ids,
    route_weights,
    expert_inputs,
    gate_weight,
    up_weight,
    down_weight,
    out_weight,
    gate_in,
    conv_sum,
    conv_c,
    conv_v,
    conv_taps,
):
    groups = lax.axis_size("sp")
    lanes = lax.axis_size("tp")
    capacity = expert_inputs.shape[1] // groups
    tokens, model_width = cotangent.shape
    cols = model_width // lanes
    units = gate_weight.shape[2]
    slots = groups * capacity
    channels = gate_in.shape[1]
    part_rows = model_width // groups
    if gate_weight.shape[0] != 1 or lanes & (lanes - 1):
        raise ValueError("unsupported mesh")
    direct = groups == 8
    me = lax.axis_index("sp")
    x = expert_inputs[0]
    w_gate, w_up, w_down = gate_weight[0], up_weight[0], down_weight[0]
    members = [[0], [1, 2, 3], [4, 5], [6, 7]] if direct else [list(range(groups))]
    ids, factors = route_ids.T, route_weights.T
    block = struct((capacity, cols), BF16)

    blocks = flat_call(
        functools.partial(dispatch_kernel, groups, direct),
        in_hbm(ids, factors, cotangent),
        [block] * (groups - 1) if direct else [struct((slots, cols), BF16)],
        2 * slots * tokens * cols,
        14,
        scratch=[
            pltpu.VMEM(ids.shape, jnp.int32),
            pltpu.VMEM(ids.shape, F32),
            pltpu.VMEM((tokens, cols), BF16),
            pltpu.SemaphoreType.DMA((3,)),
        ],
        space=pltpu.HBM,
    )
    w_gate, w_up, w_down, select, own_cot, *own_pieces = flat_call(
        functools.partial(local_kernel, lanes, groups, capacity, direct),
        in_hbm(ids, factors, cotangent, w_gate, w_up, w_down),
        [in_vmem(w) for w in (w_gate, w_up, w_down)]
        + [struct((tokens, slots), BF16), struct((tokens, cols), BF16)]
        + ([block] * lanes if direct else []),
        2 * slots * tokens * cols,
        14,
        scratch=[
            pltpu.VMEM(ids.shape, jnp.int32),
            pltpu.VMEM(ids.shape, F32),
            pltpu.VMEM((tokens, model_width), BF16),
            pltpu.SemaphoreType.DMA((6,)),
        ],
        space=pltpu.HBM,
    )
    half_slots = slots // 2
    halves = [
        flat_call(
            functools.partial(pre_kernel, capacity, h, direct),
            (*in_hbm(x), w_gate, w_up),
            [struct((half_slots, units), t) for t in (BF16, F32, F32)],
            4 * half_slots * model_width * units,
            12,
            scratch=[pltpu.VMEM((half_slots, model_width), BF16), pltpu.SemaphoreType.DMA((1,))],
            space=(pltpu.HBM, pltpu.VMEM, pltpu.VMEM),
        )
        for h in range(2)
    ]

    def arrive(ks):
        if not direct:
            value = blocks[0].reshape(groups, capacity, cols)
            value = lax.all_to_all(value, "sp", split_axis=0, concat_axis=0, tiled=True)
            return gather_lanes(value.reshape(slots, cols), lanes)
        if ks == [0]:
            return own_pieces
        got = [swap(blocks[k - 1], "sp", k) for k in ks]
        return gather_lanes(jnp.concatenate(got, axis=0), lanes)

    arrived = {}
    for g in reversed(range(len(members))):
        arrived[g] = arrive(members[g])

    grads, returned = {}, {}
    for g, ks in enumerate(members):
        rows = len(ks) * capacity
        which, offset = divmod(ks[0] * capacity, half_slots)
        _, slope, swish = halves[which]
        if not direct:
            slope, swish = (jnp.concatenate([h[i] for h in halves]) for i in (1, 2))
        gate, up, *parts = flat_call(
            functools.partial(mid_kernel, lanes, offset),
            (slope, swish, w_gate, w_up, w_down, *arrived[g]),
            [struct((rows, units), BF16)] * 2 + [struct((rows, cols), BF16)] * lanes,
            6 * rows * model_width * units,
            14,
        )
        grads[g] = (gate, up)
        total = sum_lanes(parts, lanes)
        if not direct:
            total = total.reshape(groups, capacity, cols)
            total = lax.all_to_all(total, "sp", split_axis=0, concat_axis=0, tiled=True)
            returned[0] = total.reshape(slots, cols)
        else:
            for i, k in enumerate(ks):
                one = total[i * capacity : (i + 1) * capacity]
                returned[k] = swap(one, "sp", k) if k else one

    count = len(members)
    places = [divmod(ks[0] * capacity, half_slots) for ks in members]
    hidden = [h[0] for h in halves] if direct else [jnp.concatenate([h[0] for h in halves])]
    flat = [piece for g in range(count) for piece in arrived[g]]
    (grad_down,) = flat_call(
        functools.partial(down_kernel, lanes, places),
        (*hidden, *flat),
        [struct((units, model_width), BF16)],
        2 * slots * model_width * units,
        16,
    )
    flat = [grad for g in range(count) for grad in grads[g]]
    grad_gate, grad_up = flat_call(
        functools.partial(gate_up_kernel, capacity, members, direct),
        (x, *flat),
        [struct((model_width, units), BF16)] * 2,
        4 * slots * model_width * units,
        28,
    )
    grad_input, kept = flat_call(
        combine_kernel,
        (select, own_cot, *[returned[k] for k in sorted(returned)]),
        [struct((tokens, cols), BF16)] * 2,
        2 * slots * tokens * cols,
        16,
    )
    pieces = gather_lanes(kept, lanes)
    part = struct((part_rows, channels), BF16)
    pair = struct((2 * part_rows, channels), BF16)
    outs = [part] * 3 + [pair] * 2 if direct else [struct((model_width, channels), BF16)]
    shapes = [
        struct((tokens, channels), BF16),
        struct((tokens, channels), F32),
        struct((part_rows, channels), F32),
    ] + outs
    grad_gate_in, grad_sum, own, *terms = flat_call(
        functools.partial(mixer_kernel, lanes, direct),
        (gate_in, conv_sum, out_weight, *pieces),
        shapes,
        4 * tokens * model_width * channels,
        16,
        scratch=[pltpu.VMEM((model_width, channels), F32)],
    )
    back = [(i, i - 1) for i in range(1, groups)]
    next_rows = lax.ppermute(grad_sum[:2], "sp", back)
    if direct:
        arrived_terms = [swap(terms[k - 1], "sp", k) for k in (1, 2, 3)]
        crossed = swap(terms[4], "sp", 1)
        stay = (terms[3].astype(F32) + crossed.astype(F32)).astype(BF16)
        for i, k in enumerate((4, 6)):
            half = stay[i * part_rows : (i + 1) * part_rows]
            arrived_terms.append(swap(half, "sp", k))
        grad_out_weight = own
        for term in arrived_terms:
            grad_out_weight = grad_out_weight + term.astype(F32)
    else:
        value = terms[0].reshape(groups, part_rows, channels)
        value = lax.all_to_all(value, "sp", split_axis=0, concat_axis=0, tiled=True)
        others = (jnp.arange(groups) != me)[:, None, None]
        grad_out_weight = own + jnp.sum(jnp.where(others, value.astype(F32), 0.0), axis=0)
    grad_conv_c, grad_conv_v = flat_call(
        conv_kernel,
        (grad_sum, next_rows, conv_taps, conv_v, conv_c),
        [struct((tokens, channels), BF16)] * 2,
        8 * tokens * channels,
        8,
    )
    return (
        grad_input,
        grad_gate[None],
        grad_up[None],
        grad_down[None],
        grad_out_weight,
        grad_gate_in,
        grad_conv_c,
        grad_conv_v,
    )


def solution(mesh):
    placed = (
        P("sp", None),
        P("sp", None),
        P("sp", None),
        P("sp", None, None),
        P("sp", None, "tp"),
        P("sp", None, "tp"),
        P("sp", "tp", None),
        P(None, "tp"),
        P("sp", "tp"),
        P("sp", "tp"),
        P("sp", "tp"),
        P("sp", "tp"),
        P(None, "tp"),
    )
    return jax.shard_map(
        body,
        mesh=mesh,
        in_specs=placed,
        out_specs=(
            P("sp", "tp"),
            P("sp", None, "tp"),
            P("sp", None, "tp"),
            P("sp", "tp", None),
            P("sp", "tp"),
            P("sp", "tp"),
            P("sp", "tp"),
            P("sp", "tp"),
        ),
        check_vma=False,
    )
```

```python
import functools
import math

import jax
import jax.numpy as jnp
from jax import lax
from jax.experimental import pallas as pl
from jax.experimental.pallas import tpu as pltpu
from jax.sharding import PartitionSpec as P


F32 = jnp.float32
BF16 = jnp.bfloat16


def dot(a, b, contract):
    return lax.dot_general(a, b, (contract, ((), ())), preferred_element_type=F32)


def swap(value, axis, distance):
    route = [(i, i ^ distance) for i in range(lax.axis_size(axis))]
    return lax.ppermute(value, axis, route)


def position(direct):
    me = lax.axis_index("sp")
    return (me if direct else 0), me, lax.axis_index("tp")


def routing(ids, weights, experts, capacity, order):
    tokens = ids.shape[1]
    slots = experts * capacity
    labels = ids[...] ^ order
    expert = lax.broadcasted_iota(jnp.int32, (experts, tokens), 0)
    hit = jnp.zeros((experts, tokens), F32)
    factor = jnp.zeros((experts, tokens), F32)
    for k in range(labels.shape[0]):
        same = expert == labels[k : k + 1]
        hit = hit + same.astype(F32)
        factor = factor + jnp.where(same, weights[k : k + 1], 0.0)
    earlier = (
        lax.broadcasted_iota(jnp.int32, (tokens, tokens), 0)
        < lax.broadcasted_iota(jnp.int32, (tokens, tokens), 1)
    ).astype(F32)
    before = dot(hit.astype(BF16), earlier.astype(BF16), ((1,), (0,))).astype(jnp.int32)
    rank = jnp.where(hit > 0, before, -1)
    row = lax.broadcasted_iota(jnp.int32, (experts, capacity, tokens), 1)
    chosen = (rank[:, None, :] == row).astype(F32)
    scale = jnp.sum(chosen * factor[:, None, :], axis=2, keepdims=True).reshape(slots, 1)
    return chosen.reshape(slots, tokens), scale


def lane_columns_of(ref, lane, cols):
    return ref.at[:, pl.ds(pl.multiple_of(lane * cols, cols), cols)]


def in_hbm(*arrays):
    return [pltpu.with_memory_space_constraint(a, pltpu.HBM) for a in arrays]


def lane_columns(ref, lane, cols):
    return ref[:, pl.ds(pl.multiple_of(lane * cols, cols), cols)]


def dispatch_kernel(experts, direct, ids_in, weights_in, cot_in, *refs):
    blocks, (ids, weights, cot, sems) = refs[:-4], refs[-4:]
    order, _, lane = position(direct)
    capacity = blocks[-1].shape[0] if direct else blocks[0].shape[0] // experts
    cols = cot.shape[1]
    copies = [
        pltpu.make_async_copy(ids_in, ids, sems.at[0]),
        pltpu.make_async_copy(weights_in, weights, sems.at[1]),
        pltpu.make_async_copy(lane_columns_of(cot_in, lane, cols), cot, sems.at[2]),
    ]
    for copy in copies:
        copy.start()
    copies[0].wait()
    copies[1].wait()
    chosen, scale = routing(ids, weights, experts, capacity, order)
    chosen = chosen.astype(BF16)
    copies[2].wait()
    if direct:
        rows = (dot(chosen[capacity:], cot[...], ((1,), (0,))) * scale[capacity:]).astype(BF16)
        for k in range(1, experts):
            blocks[k - 1][...] = rows[(k - 1) * capacity : k * capacity]
    else:
        blocks[0][...] = (dot(chosen, cot[...], ((1,), (0,))) * scale).astype(BF16)


def local_kernel(lanes, experts, capacity, direct, ids_in, weights_in, cot_in, *refs):
    sources, targets = refs[:3], refs[3:6]
    select, own_cot, *pieces = refs[6:-4]
    ids, weights, cot, sems = refs[-4:]
    order, _, lane = position(direct)
    cols = cot.shape[1] // lanes
    copies = [
        pltpu.make_async_copy(ids_in, ids, sems.at[0]),
        pltpu.make_async_copy(weights_in, weights, sems.at[1]),
        pltpu.make_async_copy(cot_in, cot, sems.at[2]),
    ]
    moves = [pltpu.make_async_copy(u, v, sems.at[3 + i]) for i, (u, v) in enumerate(zip(sources, targets))]
    for copy in copies + moves:
        copy.start()
    for copy in copies:
        copy.wait()
    chosen, scale = routing(ids, weights, experts, capacity, order)
    select[...] = chosen.T.astype(BF16)
    own_cot[...] = lane_columns(cot, lane, cols)
    if direct:
        first = chosen[:capacity].astype(BF16)
        for j in range(lanes):
            rows = dot(first, lane_columns(cot, lane ^ j, cols), ((1,), (0,)))
            pieces[j][...] = (rows * scale[:capacity]).astype(BF16)
    for move in moves:
        move.wait()


def pre_kernel(capacity, half, direct, x_in, w_gate, w_up, hidden, slope, swish, x, sem):
    order, _, _ = position(direct)
    rows = x.shape[0]
    pack = rows // capacity
    start = pl.multiple_of(((order // pack) ^ half) * rows, rows)
    copy = pltpu.make_async_copy(x_in.at[pl.ds(start, rows)], x, sem.at[0])
    copy.start()
    copy.wait()
    gate = dot(x[...], w_gate[...], ((1,), (0,)))
    up = dot(x[...], w_up[...], ((1,), (0,)))
    sig = jax.nn.sigmoid(gate)
    silu = gate * sig
    deriv = up * sig * (1.0 + gate * (1.0 - sig))
    keep = (silu * up).astype(BF16)
    for i in range(pack):
        part = slice(i * capacity, (i + 1) * capacity)
        place = ((order ^ i) & (pack - 1)) * capacity
        spot = pl.ds(pl.multiple_of(place, capacity), capacity)
        hidden[spot, :] = keep[part]
        slope[spot, :] = deriv[part]
        swish[spot, :] = silu[part]


def mid_kernel(lanes, first, slope, swish, w_gate, w_up, w_down, *refs):
    pieces, (d_gate, d_up), outs = refs[:lanes], refs[lanes : lanes + 2], refs[lanes + 2 :]
    rows, cols = pieces[0].shape
    lane = lax.axis_index("tp")
    part = slice(first, first + rows)
    total = None
    for j in range(lanes):
        term = dot(pieces[j][...], lane_columns(w_down, lane ^ j, cols), ((1,), (1,)))
        total = term if total is None else total + term
    gate = (total * slope[part, :]).astype(BF16)
    up = (total * swish[part, :]).astype(BF16)
    d_gate[...] = gate
    d_up[...] = up
    for j in range(lanes):
        spot = pl.ds(pl.multiple_of((lane ^ j) * cols, cols), cols)
        out = dot(gate, w_gate[spot, :], ((1,), (1,))) + dot(up, w_up[spot, :], ((1,), (1,)))
        outs[j][...] = out.astype(BF16)


def down_kernel(lanes, places, *refs):
    count = 1 + max(which for which, _ in places)
    hidden, pieces, out = refs[:count], refs[count:-1], refs[-1]
    cols = out.shape[1] // lanes
    lane = lax.axis_index("tp")
    for j in range(lanes):
        total = None
        for g, (which, start) in enumerate(places):
            piece = pieces[g * lanes + j]
            rows = hidden[which][start : start + piece.shape[0]]
            term = dot(rows, piece[...], ((0,), (0,)))
            total = term if total is None else total + term
        spot = pl.ds(pl.multiple_of((lane ^ j) * cols, cols), cols)
        out[:, spot] = total.astype(BF16)


def conv_kernel(d_sum, following, taps, conv_v, conv_c, d_conv_c, d_conv_v):
    value = d_sum[...]
    last = value.shape[0] - 1
    row = lax.broadcasted_iota(jnp.int32, value.shape, 0)
    once = jnp.where(row == last, following[0:1], pltpu.roll(value, last, 0))
    twice = jnp.where(row == last, following[1:2], pltpu.roll(once, last, 0))
    total = taps[0:1] * twice + taps[1:2] * once + taps[2:3] * value
    d_conv_c[...] = (total * conv_v[...].astype(F32)).astype(BF16)
    d_conv_v[...] = (total * conv_c[...].astype(F32)).astype(BF16)


def in_vmem(array):
    return pltpu.VMEM(array.shape, array.dtype)


def gate_up_kernel(capacity, members, direct, x, *refs):
    grads, (out_gate, out_up) = refs[:-2], refs[-2:]
    order, _, _ = position(direct)
    gates, ups = {}, {}
    for g, ks in enumerate(members):
        for i, k in enumerate(ks):
            part = slice(i * capacity, (i + 1) * capacity)
            gates[k] = grads[2 * g][part]
            ups[k] = grads[2 * g + 1][part]

    def paired(values, k):
        low, high = values[k], values[k + 1]
        if not direct:
            return jnp.concatenate([low, high], axis=0)
        odd = (order & 1) == 1
        return jnp.concatenate([jnp.where(odd, high, low), jnp.where(odd, low, high)], axis=0)

    for values, out in ((gates, out_gate), (ups, out_up)):
        total = None
        for k in range(0, len(values), 2):
            start = pl.multiple_of(((order // 2) ^ (k // 2)) * 2 * capacity, 2 * capacity)
            term = dot(x[pl.ds(start, 2 * capacity), :], paired(values, k), ((0,), (0,)))
            total = term if total is None else total + term
        out[...] = total.astype(BF16)


def combine_kernel(starts, select, base, *refs):
    blocks, outs = refs[: len(starts)], refs[len(starts) :]
    total = base[...].astype(F32)
    for start, block in zip(starts, blocks):
        size = block.shape[0]
        total = total + dot(select[:, start : start + size], block[...], ((1,), (0,)))
    for out in outs:
        out[...] = total.astype(out.dtype)


def mixer_kernel(lanes, direct, gate_in, conv_sum, w_out, *refs):
    pieces = refs[:lanes]
    d_gate_in, d_sum = refs[lanes : lanes + 2]
    own, outs, scratch = refs[lanes + 2], refs[lanes + 3 : -1], refs[-1]
    cols = pieces[0].shape[1]
    order, me, lane = position(direct)
    gate = gate_in[...].astype(F32)
    conv = conv_sum[...].astype(F32)
    mixed = (gate * conv).astype(BF16)
    total = None
    for j in range(lanes):
        spot = pl.ds(pl.multiple_of((lane ^ j) * cols, cols), cols)
        piece = pieces[j][...]
        term = dot(piece, w_out[spot, :], ((1,), (0,)))
        total = term if total is None else total + term
        scratch[spot, :] = dot(piece, mixed, ((0,), (0,)))
    d_gate_in[...] = (total * conv).astype(BF16)
    d_sum[...] = total * gate
    size = own.shape[0]
    if direct:

        def part(k):
            return scratch[pl.ds(pl.multiple_of((order ^ k) * size, size), size), :]

        own[...] = part(0)
        near, stay, cross = outs[:3], outs[3], outs[4]
        for k in (1, 2, 3):
            near[k - 1][...] = part(k).astype(BF16)
        for i, k in enumerate((4, 6)):
            spot = slice(i * size, (i + 1) * size)
            stay[spot] = part(k).astype(BF16)
            cross[spot] = part(k ^ 1).astype(BF16)
    else:
        own[...] = scratch[pl.ds(pl.multiple_of(me * size, size), size), :]
        outs[0][...] = scratch[...].astype(BF16)


def flat_call(kernel, ins, outs, flops, limit, scratch=(), space=pltpu.VMEM):
    return pl.pallas_call(
        kernel,
        in_specs=[
            pl.BlockSpec(memory_space=space[i] if isinstance(space, tuple) else space)
            for i in range(len(ins))
        ],
        out_specs=[pl.BlockSpec(memory_space=pltpu.VMEM)] * len(outs),
        out_shape=outs,
        scratch_shapes=list(scratch),
        compiler_params=pltpu.CompilerParams(vmem_limit_bytes=limit << 20),
        cost_estimate=pl.CostEstimate(
            flops=flops,
            transcendentals=0,
            bytes_accessed=sum(math.prod(a.shape) * a.dtype.itemsize for a in [*ins, *outs]),
        ),
    )(*ins)


def struct(shape, dtype):
    return jax.ShapeDtypeStruct(shape, dtype)


def spread(have, lanes, distance):
    while distance >= 1:
        for j in list(have):
            k = j ^ distance
            have[k] = swap(have[j], "tp", distance)
        distance //= 2
    return [have[j] for j in range(lanes)]


def gather_lanes(own, lanes):
    return spread({0: own}, lanes, lanes // 2)


def sum_lanes(parts, lanes):
    have = {j: parts[j].astype(F32) for j in range(lanes)}
    distance = 1
    while distance < lanes:
        sent = {j: swap(have[j].astype(BF16), "tp", distance) for j in have if j & distance}
        have = {
            j: have[j] + sent[j ^ distance].astype(F32) for j in have if not j & distance
        }
        distance *= 2
    return have[0].astype(BF16)


def body(
    cotangent,
    route_ids,
    route_weights,
    expert_inputs,
    gate_weight,
    up_weight,
    down_weight,
    out_weight,
    gate_in,
    conv_sum,
    conv_c,
    conv_v,
    conv_taps,
):
    groups = lax.axis_size("sp")
    lanes = lax.axis_size("tp")
    capacity = expert_inputs.shape[1] // groups
    tokens, model_width = cotangent.shape
    cols = model_width // lanes
    units = gate_weight.shape[2]
    slots = groups * capacity
    channels = gate_in.shape[1]
    part_rows = model_width // groups
    if gate_weight.shape[0] != 1 or lanes & (lanes - 1):
        raise ValueError("unsupported mesh")
    direct = groups == 8
    me = lax.axis_index("sp")
    x = expert_inputs[0]
    w_gate, w_up, w_down = gate_weight[0], up_weight[0], down_weight[0]
    members = [[0], [1, 2, 3], [4, 5], [6, 7]] if direct else [list(range(groups))]
    ids, factors = route_ids.T, route_weights.T
    block = struct((capacity, cols), BF16)

    blocks = flat_call(
        functools.partial(dispatch_kernel, groups, direct),
        in_hbm(ids, factors, cotangent),
        [block] * (groups - 1) if direct else [struct((slots, cols), BF16)],
        2 * slots * tokens * cols,
        14,
        scratch=[
            pltpu.VMEM(ids.shape, jnp.int32),
            pltpu.VMEM(ids.shape, F32),
            pltpu.VMEM((tokens, cols), BF16),
            pltpu.SemaphoreType.DMA((3,)),
        ],
        space=pltpu.HBM,
    )
    w_gate, w_up, w_down, select, own_cot, *own_pieces = flat_call(
        functools.partial(local_kernel, lanes, groups, capacity, direct),
        in_hbm(ids, factors, cotangent, w_gate, w_up, w_down),
        [in_vmem(w) for w in (w_gate, w_up, w_down)]
        + [struct((tokens, slots), BF16), struct((tokens, cols), BF16)]
        + ([block] * lanes if direct else []),
        2 * slots * tokens * cols,
        14,
        scratch=[
            pltpu.VMEM(ids.shape, jnp.int32),
            pltpu.VMEM(ids.shape, F32),
            pltpu.VMEM((tokens, model_width), BF16),
            pltpu.SemaphoreType.DMA((6,)),
        ],
        space=pltpu.HBM,
    )
    half_slots = slots // 2
    halves = [
        flat_call(
            functools.partial(pre_kernel, capacity, h, direct),
            (*in_hbm(x), w_gate, w_up),
            [struct((half_slots, units), t) for t in (BF16, F32, F32)],
            4 * half_slots * model_width * units,
            12,
            scratch=[pltpu.VMEM((half_slots, model_width), BF16), pltpu.SemaphoreType.DMA((1,))],
            space=(pltpu.HBM, pltpu.VMEM, pltpu.VMEM),
        )
        for h in range(2)
    ]

    def arrive(ks):
        if not direct:
            value = blocks[0].reshape(groups, capacity, cols)
            value = lax.all_to_all(value, "sp", split_axis=0, concat_axis=0, tiled=True)
            return gather_lanes(value.reshape(slots, cols), lanes)
        if ks == [0]:
            return own_pieces
        got = [swap(blocks[k - 1], "sp", k) for k in ks]
        return gather_lanes(jnp.concatenate(got, axis=0), lanes)

    arrived = {}
    for g in reversed(range(len(members))):
        arrived[g] = arrive(members[g])

    grads, returned = {}, {}
    for g, ks in enumerate(members):
        rows = len(ks) * capacity
        which, offset = divmod(ks[0] * capacity, half_slots)
        _, slope, swish = halves[which]
        if not direct:
            slope, swish = (jnp.concatenate([h[i] for h in halves]) for i in (1, 2))
        gate, up, *parts = flat_call(
            functools.partial(mid_kernel, lanes, offset),
            (slope, swish, w_gate, w_up, w_down, *arrived[g]),
            [struct((rows, units), BF16)] * 2 + [struct((rows, cols), BF16)] * lanes,
            6 * rows * model_width * units,
            14,
        )
        grads[g] = (gate, up)
        total = sum_lanes(parts, lanes)
        if not direct:
            total = total.reshape(groups, capacity, cols)
            total = lax.all_to_all(total, "sp", split_axis=0, concat_axis=0, tiled=True)
            returned[0] = total.reshape(slots, cols)
        else:
            for i, k in enumerate(ks):
                one = total[i * capacity : (i + 1) * capacity]
                returned[k] = swap(one, "sp", k) if k else one

    count = len(members)
    places = [divmod(ks[0] * capacity, half_slots) for ks in members]
    hidden = [h[0] for h in halves] if direct else [jnp.concatenate([h[0] for h in halves])]
    flat = [piece for g in range(count) for piece in arrived[g]]
    (grad_down,) = flat_call(
        functools.partial(down_kernel, lanes, places),
        (*hidden, *flat),
        [struct((units, model_width), BF16)],
        2 * slots * model_width * units,
        16,
    )
    flat = [grad for g in range(count) for grad in grads[g]]
    grad_gate, grad_up = flat_call(
        functools.partial(gate_up_kernel, capacity, members, direct),
        (x, *flat),
        [struct((model_width, units), BF16)] * 2,
        4 * slots * model_width * units,
        28,
    )
    soon = [k for k in (0, 4, 5) if k in returned] if direct else []
    late = [k for k in sorted(returned) if k not in soon]
    base = own_cot
    if soon:
        (base,) = flat_call(
            functools.partial(combine_kernel, [k * capacity for k in soon]),
            (select, own_cot, *[returned[k] for k in soon]),
            [struct((tokens, cols), F32)],
            2 * len(soon) * capacity * tokens * cols,
            16,
        )
    grad_input, kept = flat_call(
        functools.partial(combine_kernel, [k * capacity for k in late]),
        (select, base, *[returned[k] for k in late]),
        [struct((tokens, cols), BF16)] * 2,
        2 * slots * tokens * cols,
        16,
    )
    pieces = gather_lanes(kept, lanes)
    part = struct((part_rows, channels), BF16)
    pair = struct((2 * part_rows, channels), BF16)
    outs = [part] * 3 + [pair] * 2 if direct else [struct((model_width, channels), BF16)]
    shapes = [
        struct((tokens, channels), BF16),
        struct((tokens, channels), F32),
        struct((part_rows, channels), F32),
    ] + outs
    grad_gate_in, grad_sum, own, *terms = flat_call(
        functools.partial(mixer_kernel, lanes, direct),
        (gate_in, conv_sum, out_weight, *pieces),
        shapes,
        4 * tokens * model_width * channels,
        16,
        scratch=[pltpu.VMEM((model_width, channels), F32)],
    )
    back = [(i, i - 1) for i in range(1, groups)]
    next_rows = lax.ppermute(grad_sum[:2], "sp", back)
    if direct:
        arrived_terms = [swap(terms[k - 1], "sp", k) for k in (1, 2, 3)]
        crossed = swap(terms[4], "sp", 1)
        stay = (terms[3].astype(F32) + crossed.astype(F32)).astype(BF16)
        for i, k in enumerate((4, 6)):
            half = stay[i * part_rows : (i + 1) * part_rows]
            arrived_terms.append(swap(half, "sp", k))
        grad_out_weight = own
        for term in arrived_terms:
            grad_out_weight = grad_out_weight + term.astype(F32)
    else:
        value = terms[0].reshape(groups, part_rows, channels)
        value = lax.all_to_all(value, "sp", split_axis=0, concat_axis=0, tiled=True)
        others = (jnp.arange(groups) != me)[:, None, None]
        grad_out_weight = own + jnp.sum(jnp.where(others, value.astype(F32), 0.0), axis=0)
    grad_conv_c, grad_conv_v = flat_call(
        conv_kernel,
        (grad_sum, next_rows, conv_taps, conv_v, conv_c),
        [struct((tokens, channels), BF16)] * 2,
        8 * tokens * channels,
        8,
    )
    return (
        grad_input,
        grad_gate[None],
        grad_up[None],
        grad_down[None],
        grad_out_weight,
        grad_gate_in,
        grad_conv_c,
        grad_conv_v,
    )


def solution(mesh):
    placed = (
        P("sp", None),
        P("sp", None),
        P("sp", None),
        P("sp", None, None),
        P("sp", None, "tp"),
        P("sp", None, "tp"),
        P("sp", "tp", None),
        P(None, "tp"),
        P("sp", "tp"),
        P("sp", "tp"),
        P("sp", "tp"),
        P("sp", "tp"),
        P(None, "tp"),
    )
    return jax.shard_map(
        body,
        mesh=mesh,
        in_specs=placed,
        out_specs=(
            P("sp", "tp"),
            P("sp", None, "tp"),
            P("sp", None, "tp"),
            P("sp", "tp", None),
            P("sp", "tp"),
            P("sp", "tp"),
            P("sp", "tp"),
            P("sp", "tp"),
        ),
        check_vma=False,
    )
```
